32 devices in a mesh: sp: 8 (over z, y), tp: 4 (over x, core).
Axes of the slice: x: 2, y: 2, z: 4, core: 2. Of those that a mesh axis runs over, the one named last changes fastest.
Arguments:
- skip_stream: bfloat16 [6144, 2048], P(('sp', 'tp')), may hold values from -24 to 24
- acceptance_signal: bfloat16 [6144, 2048], P('sp', 'tp'), may hold values from -6 to 6
- lookup_mapped: bfloat16 [6144, 2048], P('sp', 'tp'), may hold values from -12 to 12
- payload_mapped: bfloat16 [6144, 2048], P('sp', 'tp'), may hold values from -6 to 6
- result_switch: bfloat16 [6144, 2048], P('sp', 'tp'), may hold values from -6 to 6
- forget_dynamic_share: bfloat16 [6144, 2048], P('sp', 'tp'), may hold values from -4 to 4
- additive_forget_logarithm: float32 [6144, 32], P('sp', 'tp'), may hold values from -1 to 0
- forget_feature_offset: float32 [2048], P('tp'), may hold values from -11 to -3
- substitution_dynamic_share: bfloat16 [6144, 2048], P('sp', 'tp'), may hold values from -6 to 6
- substitution_feature_offset: float32 [2048], P('tp'), may hold values from -6.5 to 2.5
- diagonal_reward_scales: float32 [2048], P('tp'), may hold values from -0.9 to 0.9
- result_matrix: bfloat16 [2048, 2048], P('tp'), may hold values from -0.125 to 0.125
- mlp_rescaler: float32 [2048], replicated, may hold values from 0.1 to 1.9
- switch_matrix: bfloat16 [2048, 5120], P('sp', 'tp'), may hold values from -0.125 to 0.125
- expand_matrix: bfloat16 [2048, 5120], P('sp', 'tp'), may hold values from -0.125 to 0.125
- contract_matrix: bfloat16 [2048, 5120], P('sp', 'tp'), may hold values from -0.25 to 0.25
Outputs:
- mixed_out: bfloat16 [6144, 2048], P(('sp', 'tp'))
The draws below stay inside these ranges and needn't reach their ends.
All inputs are finite; a program needn't handle non-finite values.
Results may differ from the reference program's by a relative error of at most 0.015.
Values may be sent and summed in bfloat16 or wider, within the bound.
A program may use at most 128 MiB of HBM per device.

```python
import jax
import jax.numpy as jnp
from jax import lax

EMBED_DIMENSION = 2048
PER_GROUP_DIMS = 64
FF = 5120
TOK_DEV = 768
TOKENS = 6144
N_TP = 4


def draw_skip_stream(key, part):
    entries = jnp.clip(jax.random.normal(jax.random.fold_in(key, 11), (TOKENS, EMBED_DIMENSION), jnp.float32), -4.0, 4.0)
    column_scale = jnp.exp(jnp.linspace(jnp.log(0.3), jnp.log(3.0), EMBED_DIMENSION))
    row_scale = jnp.exp(jax.random.uniform(jax.random.fold_in(key, 12), (TOKENS, 1), jnp.float32, jnp.log(0.5), jnp.log(2.0)))
    return (entries * column_scale[None, :] * row_scale).astype(jnp.bfloat16)


def draw_lookup_mapped(key, part):
    attention_groups = EMBED_DIMENSION // PER_GROUP_DIMS
    direction = jnp.clip(jax.random.normal(jax.random.fold_in(key, 51), (attention_groups, PER_GROUP_DIMS), jnp.float32), -4.0, 4.0)
    noise = jnp.clip(jax.random.normal(jax.random.fold_in(key, 52), (TOKENS, attention_groups, PER_GROUP_DIMS), jnp.float32), -4.0, 4.0)
    weight = 2.0 * jnp.ones((attention_groups, 1), jnp.float32)
    shared = weight * direction
    return (noise + shared[None, :, :]).reshape(TOKENS, EMBED_DIMENSION).astype(jnp.bfloat16)


def draw_forget_dynamic_share(key, part):
    blocks = TOKENS // TOK_DEV
    offset = jax.random.uniform(jax.random.fold_in(key, 21), (blocks, 1, 1), jnp.float32, -0.7, 0.7)
    noise = jnp.clip(jax.random.normal(jax.random.fold_in(key, 22), (blocks, TOK_DEV, EMBED_DIMENSION), jnp.float32), -3.0, 3.0)
    return (noise + offset).reshape(TOKENS, EMBED_DIMENSION).astype(jnp.bfloat16)


def draw_additive_forget_logarithm(key, part):
    spots = jax.random.randint(jax.random.fold_in(key, 31), (4,), 0, TOKENS)
    struck = jnp.any(jnp.arange(TOKENS)[:, None] == spots[None, :], axis=1)
    losses = jnp.log(jax.random.uniform(jax.random.fold_in(key, 32), (TOKENS, EMBED_DIMENSION // PER_GROUP_DIMS), jnp.float32, 0.5, 0.8))
    return jnp.where(struck[:, None], losses, 0.0).astype(jnp.float32)


def draw_forget_feature_offset(key, part):
    attention_groups = EMBED_DIMENSION // PER_GROUP_DIMS
    fast_share = 0.5
    quick_heads = jax.random.uniform(jax.random.fold_in(key, 41), (attention_groups, 1), jnp.float32) < fast_share
    quick = jax.random.uniform(jax.random.fold_in(key, 42), (attention_groups, PER_GROUP_DIMS), jnp.float32, -4.5, -3.0)
    patient = jax.random.uniform(jax.random.fold_in(key, 43), (attention_groups, PER_GROUP_DIMS), jnp.float32, -11.0, -9.0)
    return jnp.where(quick_heads, quick, patient).reshape(EMBED_DIMENSION).astype(jnp.float32)


def draw_substitution_feature_offset(key, part):
    attention_groups = EMBED_DIMENSION // PER_GROUP_DIMS
    order = jax.random.permutation(jax.random.fold_in(key, 61), attention_groups)
    levels = jnp.linspace(-6.0, 2.2, attention_groups)
    jitter = jax.random.uniform(jax.random.fold_in(key, 62), (attention_groups, PER_GROUP_DIMS), jnp.float32, -0.3, 0.3)
    return (levels[order][:, None] + jitter).reshape(EMBED_DIMENSION).astype(jnp.float32)


def steps_of(key, dims, split, least, top_value):
    gain = 1.0
    for dim, shards_of in split:
        steps = jax.random.uniform(jax.random.fold_in(jax.random.fold_in(key, 6), dim), (shards_of,), jnp.float32, least / len(split), top_value / len(split))
        gain = gain * jnp.repeat(jnp.exp(steps), dims[dim] // shards_of).reshape((-1,) + (1,) * (len(dims) - 1 - dim))
    return gain


def scatter_about(key, dims, scale, limit, cuts=(), kind=jnp.bfloat16):
    values = scale * jax.random.normal(key, dims, jnp.float32)
    if cuts:
        values = values * steps_of(key, dims, cuts, -0.22, 0.18)
    return jnp.clip(values, -limit, limit).astype(kind)


def setup_inputs(seed: int = 0) -> dict:
    seeds = jax.random.split(jax.random.key(seed), 17)
    skip_stream = draw_skip_stream(jax.random.fold_in(seeds[16], 71), 0)
    acceptance_signal = scatter_about(seeds[1], (TOKENS, EMBED_DIMENSION), 1.0, 6.0, ((0, 8), (1, 4)))
    lookup_mapped = draw_lookup_mapped(jax.random.fold_in(seeds[16], 71), 0)
    payload_mapped = scatter_about(seeds[3], (TOKENS, EMBED_DIMENSION), 1.0, 6.0, ((0, 8), (1, 4)))
    result_switch = scatter_about(seeds[4], (TOKENS, EMBED_DIMENSION), 1.0, 6.0, ((0, 8), (1, 4)))
    forget_dynamic_share = draw_forget_dynamic_share(jax.random.fold_in(seeds[16], 71), 0)
    additive_forget_logarithm = draw_additive_forget_logarithm(jax.random.fold_in(seeds[16], 71), 0)
    forget_feature_offset = draw_forget_feature_offset(jax.random.fold_in(seeds[16], 71), 0)
    substitution_dynamic_share = scatter_about(seeds[8], (TOKENS, EMBED_DIMENSION), 1.0, 6.0, ((0, 8), (1, 4)))
    substitution_feature_offset = draw_substitution_feature_offset(jax.random.fold_in(seeds[16], 71), 0)
    diagonal_reward_scales = scatter_about(seeds[10], (EMBED_DIMENSION,), 0.15, 0.9, ((0, 4),), jnp.float32)
    result_matrix = scatter_about(seeds[11], (EMBED_DIMENSION, EMBED_DIMENSION), EMBED_DIMENSION ** -0.5, 0.125, ((0, 4),))
    mlp_rescaler = jnp.clip(1.0 + 0.18 * jax.random.normal(seeds[12], (EMBED_DIMENSION,), jnp.float32), 0.1, 1.9)
    switch_matrix = scatter_about(seeds[13], (EMBED_DIMENSION, FF), EMBED_DIMENSION ** -0.5, 0.125, ((0, 8), (1, 4)))
    expand_matrix = scatter_about(seeds[14], (EMBED_DIMENSION, FF), EMBED_DIMENSION ** -0.5, 0.125, ((0, 8), (1, 4)))
    contract_matrix = scatter_about(seeds[15], (EMBED_DIMENSION, FF), (FF // 8) ** -0.5, 0.25, ((0, 8), (1, 4)))
    return dict(skip_stream=skip_stream, acceptance_signal=acceptance_signal, lookup_mapped=lookup_mapped, payload_mapped=payload_mapped, result_switch=result_switch, forget_dynamic_share=forget_dynamic_share, additive_forget_logarithm=additive_forget_logarithm, forget_feature_offset=forget_feature_offset, substitution_dynamic_share=substitution_dynamic_share, substitution_feature_offset=substitution_feature_offset, diagonal_reward_scales=diagonal_reward_scales, result_matrix=result_matrix, mlp_rescaler=mlp_rescaler, switch_matrix=switch_matrix, expand_matrix=expand_matrix, contract_matrix=contract_matrix)


norm_eps = 1e-06
group_eps = 0.00064
half_step = 0.5

def group_sum(left, right, groups):
    span = left.shape[1] // groups

    def add_group(total, index):
        first = (index * span).astype(jnp.int32)
        left_part = lax.dynamic_slice_in_dim(left, first, span, 1)
        right_part = lax.dynamic_slice_in_dim(right, first, span, 0)
        partial_prod = jnp.dot(left_part, right_part, preferred_element_type=jnp.float32)
        partial_prod = lax.optimization_barrier(partial_prod.astype(jnp.bfloat16)).astype(jnp.float32)
        return (total + partial_prod, None)
    start_total = jnp.zeros((left.shape[0], right.shape[1]), jnp.float32)
    total, _ = lax.scan(add_group, start_total, jnp.arange(groups, dtype=jnp.int32))
    return total.astype(jnp.bfloat16)

def advance(memory, inputs):
    read_now, decay_now, key_now, value_now, unit_now, rate_now = inputs
    recall = lax.optimization_barrier(jnp.sum(memory * unit_now[:, None, :], axis=-1))
    memory = memory * decay_now[:, None, :] - recall[:, :, None] * (unit_now * rate_now)[:, None, :] + value_now[:, :, None] * key_now[:, None, :]
    return (memory, lax.optimization_barrier(jnp.sum(memory * read_now[:, None, :], axis=-1)))

def reference(skip_stream, acceptance_signal, lookup_mapped, payload_mapped, result_switch, forget_dynamic_share, additive_forget_logarithm, forget_feature_offset, substitution_dynamic_share, substitution_feature_offset, diagonal_reward_scales, result_matrix, mlp_rescaler, switch_matrix, expand_matrix, contract_matrix):
    sequence_span = skip_stream.shape[0]
    attention_groups = EMBED_DIMENSION // PER_GROUP_DIMS

    def by_head(values):
        return values.astype(jnp.float32).reshape(sequence_span, attention_groups, PER_GROUP_DIMS)
    acceptance_lines = by_head(acceptance_signal)
    lookup_vectors = by_head(lookup_mapped)
    payload_vectors = by_head(payload_mapped)
    log_decay_rate = -jax.nn.softplus(-(forget_feature_offset[None, :] + forget_dynamic_share.astype(jnp.float32))) - 0.5
    decay_factor_step = jnp.exp(-jnp.exp(log_decay_rate).reshape(sequence_span, attention_groups, PER_GROUP_DIMS) + additive_forget_logarithm[:, :, None])
    replace_rate = jax.nn.sigmoid(substitution_feature_offset[None, :] + substitution_dynamic_share.astype(jnp.float32))
    replace_rate = replace_rate.reshape(sequence_span, attention_groups, PER_GROUP_DIMS)
    unit_key = lookup_vectors * lax.rsqrt(lax.optimization_barrier(jnp.sum(lookup_vectors * lookup_vectors, axis=-1, keepdims=True)) + norm_eps)
    start_memory = jnp.zeros((attention_groups, PER_GROUP_DIMS, PER_GROUP_DIMS), jnp.float32)
    _, outcome = lax.scan(advance, start_memory, (acceptance_lines, decay_factor_step, lookup_vectors, payload_vectors, unit_key, replace_rate))
    centre = lax.optimization_barrier(jnp.mean(outcome, axis=-1, keepdims=True))
    spread = lax.optimization_barrier(jnp.mean(jnp.square(outcome - centre), axis=-1, keepdims=True))
    rescaled_attention = (outcome - centre) * lax.rsqrt(spread + group_eps)
    diagonal_reward_summand = lax.optimization_barrier(jnp.sum(acceptance_lines * lookup_vectors * diagonal_reward_scales.reshape(attention_groups, PER_GROUP_DIMS), axis=-1, keepdims=True)) * payload_vectors
    merged_attention = ((rescaled_attention + diagonal_reward_summand).reshape(sequence_span, EMBED_DIMENSION) * result_switch.astype(jnp.float32)).astype(jnp.bfloat16)
    projected = group_sum(merged_attention, result_matrix, N_TP)
    stream = skip_stream.astype(jnp.float32) + projected.astype(jnp.float32)
    scale_rows = lax.rsqrt(lax.optimization_barrier(jnp.mean(stream * stream, axis=-1, keepdims=True)) + norm_eps)
    normed_rows = (stream * scale_rows * mlp_rescaler[None, :]).astype(jnp.bfloat16)
    gate_act = jnp.dot(normed_rows, switch_matrix, preferred_element_type=jnp.float32)
    up_act = jnp.dot(normed_rows, expand_matrix, preferred_element_type=jnp.float32)
    hidden = (jax.nn.silu(gate_act) * up_act).astype(jnp.bfloat16)
    ffn_out = group_sum(hidden, contract_matrix.T, N_TP)
    return (stream + half_step * ffn_out.astype(jnp.float32)).astype(jnp.bfloat16)
```

```python
import functools

import jax
import jax.numpy as jnp
from jax import lax
from jax.experimental import pallas as pl
from jax.experimental.pallas import tpu as pltpu
from jax.sharding import PartitionSpec as P

PER_GROUP_DIMS = 64


norm_eps = 1e-06
group_eps = 0.00064
half_step = 0.5
exact = lax.Precision.HIGHEST

PAIR = 2 * PER_GROUP_DIMS
CHUNK = 64
ROWS_OUT = 256
NT = (((1,), (1,)), ((), ()))
NN = (((1,), (0,)), ((), ()))
TN = (((0,), (0,)), ((), ()))
bf16 = jnp.bfloat16
f32 = jnp.float32
P_SCORE, P_INV, P_SOLVE, P_OUT, P_STATE = 3, 1, 3, 3, 1


def mm(left, right, dims, passes):
    if passes == 6:
        return lax.dot_general(left, right, dims, precision=exact, preferred_element_type=f32)
    left_hi, right_hi = left.astype(bf16), right.astype(bf16)
    total = lax.dot_general(left_hi, right_hi, dims, preferred_element_type=f32)
    if passes == 3:
        left_lo = (left - left_hi.astype(f32)).astype(bf16)
        right_lo = (right - right_hi.astype(f32)).astype(bf16)
        total += lax.dot_general(left_hi, right_lo, dims, preferred_element_type=f32)
        total += lax.dot_general(left_lo, right_hi, dims, preferred_element_type=f32)
    return total


def halves(shape):
    return lax.broadcasted_iota(jnp.int32, shape, 1) < PER_GROUP_DIMS


def stack(values):
    first = halves(values.shape)
    zero = jnp.zeros_like(values)
    return jnp.concatenate([jnp.where(first, values, zero), jnp.where(first, zero, values)], 0)


def fold(values):
    size = values.shape[0] // 2
    return values[:size] + values[size:]


def head_sums(values):
    row = lax.broadcasted_iota(jnp.int32, (PAIR, PAIR), 0) // PER_GROUP_DIMS
    col = lax.broadcasted_iota(jnp.int32, (PAIR, PAIR), 1) // PER_GROUP_DIMS
    ones = jnp.where(row == col, 1.0, 0.0).astype(bf16)
    hi = values.astype(bf16)
    left = values - hi.astype(f32)
    mid = left.astype(bf16)
    low = (left - mid.astype(f32)).astype(bf16)
    return (
        jnp.dot(hi, ones, preferred_element_type=f32)
        + jnp.dot(mid, ones, preferred_element_type=f32)
        + jnp.dot(low, ones, preferred_element_type=f32)
    )


def advance_chunk(
    here, read_ref, key_ref, value_ref, forget_ref, added_ref, rate_ref, forget_off_ref,
    rate_off_ref, local_ref, coef_ref, memory,
):
    pairs = read_ref.shape[1] // PAIR
    span = range(pairs)
    row = lax.broadcasted_iota(jnp.int32, (PAIR, PAIR), 0)
    col = lax.broadcasted_iota(jnp.int32, (PAIR, PAIR), 1)
    diagonal = jnp.where(row == col, 1.0, 0.0)
    same_head = (row // CHUNK) == (col // CHUNK)
    strict = same_head & (col < row)
    inclusive = same_head & (col <= row)

    lower = (
        lax.broadcasted_iota(jnp.int32, (CHUNK, CHUNK), 1)
        <= lax.broadcasted_iota(jnp.int32, (CHUNK, CHUNK), 0)
    )
    lower = jnp.where(lower, 1.0, 0.0)
    first = halves((CHUNK, PAIR))
    at = [slice(p * PAIR, (p + 1) * PAIR) for p in span]
    decay_rate = [
        jax.nn.sigmoid(forget_off_ref[:, at[p]] + forget_ref[here, at[p]].astype(f32)) for p in span
    ]
    log_step = [
        -0.6065306597126334 * decay_rate[p]
        + jnp.where(first, added_ref[here, 2 * p : 2 * p + 1], added_ref[here, 2 * p + 1 : 2 * p + 2])
        for p in span
    ]
    cumulate = [mm(lower, log_step[p], NN, 6) for p in span]
    key = [key_ref[here, at[p]].astype(f32) for p in span]
    unit = [key[p] * lax.rsqrt(head_sums(key[p] * key[p]) + norm_eps) for p in span]
    erase = [
        unit[p] * jax.nn.sigmoid(rate_off_ref[:, at[p]] + rate_ref[here, at[p]].astype(f32))
        for p in span
    ]
    middle = [cumulate[p][CHUNK // 2 - 1 : CHUNK // 2] for p in span]
    last = [cumulate[p][CHUNK - 1 : CHUNK] for p in span]
    growth = [jnp.exp(cumulate[p] - middle[p]) for p in span]
    shrink = [jnp.exp(middle[p] - cumulate[p]) for p in span]
    to_middle = [jnp.exp(middle[p]) for p in span]
    from_middle = [jnp.exp(last[p] - middle[p]) for p in span]
    over_chunk = [jnp.exp(last[p]) for p in span]
    before = [jnp.exp(cumulate[p] - log_step[p] - middle[p]) * unit[p] for p in span]
    read = [read_ref[here, at[p]].astype(f32) * growth[p] for p in span]
    key_back = [key[p] * shrink[p] for p in span]
    erase_back = [erase[p] * shrink[p] for p in span]
    score = [
        mm(
            jnp.concatenate([stack(before[p]), stack(read[p])], 0),
            jnp.concatenate([stack(key_back[p]), stack(erase_back[p])], 0),
            NT,
            P_SCORE,
        )
        for p in span
    ]
    key_past = [jnp.where(strict, score[p][:PAIR, :PAIR], 0.0) for p in span]
    erase_past = [jnp.where(strict, score[p][:PAIR, PAIR:], 0.0) for p in span]
    key_read = [jnp.where(inclusive, score[p][PAIR:, :PAIR], 0.0) for p in span]
    erase_read = [jnp.where(inclusive, score[p][PAIR:, PAIR:], 0.0) for p in span]
    value = [stack(value_ref[here, at[p]]).astype(f32) for p in span]
    recall = [mm(key_past[p], value[p], NN, P_SOLVE) for p in span]
    inverse = [
        diagonal - jnp.where((row // 2) == (col // 2), erase_past[p], 0.0) for p in span
    ]
    size = 2
    while size < CHUNK:
        off = ((row // (2 * size)) == (col // (2 * size))) & ((row // size) != (col // size))
        part = [mm(jnp.where(off, erase_past[p], 0.0), inverse[p], NN, P_INV) for p in span]
        inverse = [inverse[p] - mm(inverse[p], part[p], NN, P_INV) for p in span]
        size *= 2
    solved = [
        mm(
            inverse[p],
            jnp.concatenate([recall[p], stack(before[p] * to_middle[p])], 1),
            NN,
            P_SOLVE,
        )
        for p in span
    ]
    inner = [
        mm(
            jnp.concatenate([key_read[p], -erase_read[p]], 1),
            jnp.concatenate(
                [jnp.concatenate([value[p], jnp.zeros_like(value[p])], 1), solved[p]], 0
            ),
            NN,
            P_OUT,
        )
        for p in span
    ]
    local = [fold(inner[p][:, :PAIR]) for p in span]
    from_start = [fold(inner[p][:, PAIR:]) + read[p] * to_middle[p] for p in span]
    both = [memory[p] for p in span]
    passed = [mm(from_start[p], both[p], NT, P_STATE) for p in span]
    for p in span:
        local_ref[here, at[p]] = local[p] + passed[p][:, :PAIR]
        coef_ref[here, at[p]] = passed[p][:, PAIR:].astype(bf16)
    key_end = [key_back[p] * from_middle[p] for p in span]
    erase_end = [erase_back[p] * from_middle[p] for p in span]
    recalled = [fold(solved[p][:, :PAIR]) for p in span]
    carried_map = [fold(solved[p][:, PAIR:]) for p in span]
    added = [
        mm(
            jnp.concatenate([value_ref[here, at[p]].astype(f32), -recalled[p]], 0),
            jnp.concatenate([key_end[p], erase_end[p]], 0),
            TN,
            P_OUT,
        )
        for p in span
    ]
    step_map = [mm(carried_map[p], erase_end[p], TN, P_OUT) for p in span]
    for p in span:
        moved = mm(both[p], jnp.where(same_head, step_map[p], 0.0), NN, P_STATE)
        kept = both[p] * over_chunk[p] - moved
        memory[p, :PAIR] = kept[:PAIR] + jnp.where(same_head, added[p], 0.0)
        memory[p, PAIR:] = kept[PAIR:]


class Layout:
    def __init__(self, mesh):
        self.n_sp, self.n_tp = mesh.shape["sp"], mesh.shape["tp"]
        devices = list(mesh.devices.flat)
        spots = [getattr(d, "coords", None) for d in devices]
        self.lanes = self.cores = 1
        if all(s is not None for s in spots):
            self.lanes = len({s[1] for s in spots})
            self.cores = len({getattr(d, "core_on_chip", 0) for d in devices})
        if self.n_sp % self.lanes:
            self.lanes = 1
        if self.n_tp % self.cores:
            self.cores = 1
        self.planes, self.sides = self.n_sp // self.lanes, self.n_tp // self.cores


def to(**where):
    return dict(device_id=where, device_id_type=pl.DeviceIdType.MESH)


def chain(total, step):
    return mm(total, step, NN, 1) + mm(total - total.astype(bf16).astype(f32), step, NN, 1)


GATE, UP, DOWN = range(3)


class Relay:
    def __init__(self, lay, blocks, whole, send_sem, recv_sem, own_sem):
        self.lay, self.blocks, self.whole, self.own_sem = lay, blocks, whole, own_sem
        self.send_sem, self.recv_sem = send_sem, recv_sem
        me = lax.axis_index("sp")
        self.z, self.y = me // lay.lanes, lax.rem(me, lay.lanes)
        self.depth = blocks[0].shape[0]

    def slot(self, hop, lane):
        return (hop + self.lay.planes - 1) * self.lay.lanes + lane

    def held(self, hop):
        return (self.z >= hop) & (self.z < self.lay.planes + hop)

    def part(self, matrix, hop, lane):
        source = (self.z - hop) * self.lay.lanes + lax.rem(
            self.y + self.lay.lanes - lane, self.lay.lanes
        )
        first = pl.multiple_of(source * self.depth, self.depth)
        return self.whole.at[matrix, pl.ds(first, self.depth)]

    def copy(self, matrix, source, place, plane, lane):
        return pltpu.make_async_remote_copy(
            src_ref=self.blocks[matrix] if source == (0, 0) else self.part(matrix, *source),
            dst_ref=self.part(matrix, *source),
            send_sem=self.send_sem.at[matrix, self.slot(*place)],
            recv_sem=self.recv_sem.at[matrix, self.slot(*place)],
            **to(sp=plane * self.lay.lanes + lane),
        )

    def ahead(self, matrix, hop, way):
        there = self.z + way
        wanted = self.held(hop) & (there >= 0) & (there < self.lay.planes)
        return self.copy(matrix, (hop, 0), (hop + way, 0), there, self.y), wanted

    def aside(self, matrix, hop, lane):
        beside = lax.rem(self.y + lane, self.lay.lanes)
        return self.copy(matrix, (hop, 0), (hop, lane), self.z, beside), self.held(hop)

    def start(self, pair):
        pl.when(pair[1])(pair[0].start)

    def own(self, matrix):
        return pltpu.make_async_copy(
            self.blocks[matrix], self.part(matrix, 0, 0), self.own_sem.at[matrix]
        )

    def arrive(self, matrix, hop, lane):
        piece = self.part(matrix, hop, lane)
        slot = self.slot(hop, lane)
        wait = pltpu.make_async_remote_copy(
            src_ref=piece,
            dst_ref=piece,
            send_sem=self.send_sem.at[matrix, slot],
            recv_sem=self.recv_sem.at[matrix, slot],
            **to(sp=lax.axis_index("sp")),
        ).wait_recv
        pl.when(self.held(hop))(wait)

    def take(self, matrix, reach):
        for hop in (reach, -reach):
            self.arrive(matrix, hop, 0)

    def forward(self, matrix, reach):
        for way in (1, -1):
            self.start(self.ahead(matrix, way * reach, way))

    def cross(self, matrix, reach):
        for hop in (reach, -reach) if reach else (0,):
            for lane in range(1, self.lay.lanes):
                self.start(self.aside(matrix, hop, lane))

    def settle(self, matrix):
        last = self.lay.planes - 1
        for reach in range(last + 1):
            for way in (1, -1):
                if reach < last:
                    copy, wanted = self.ahead(matrix, way * reach, way)
                    pl.when(wanted)(copy.wait_send)
            for hop in (reach, -reach) if reach else (0,):
                for lane in range(1, self.lay.lanes):
                    copy, wanted = self.aside(matrix, hop, lane)
                    pl.when(wanted)(copy.wait_send)


def layer_kernel(lay, steps, *refs):
    (
        skip_ref, read_ref, key_ref, value_ref, switch_ref, forget_ref, added_ref, forget_off_ref,
        rate_ref, rate_off_ref, scales_ref, matrix_ref, gain_ref, gate_ref, up_ref, down_ref,
        out_ref,
        local_ref, coef_ref, memory, lane_ref, plane_ref, mine_ref, carried_ref, mixed, gathered,
        matrix, stream_ref, rows_ref, hidden_ref, whole, own, inner, near, outer, far,
        relay_send, relay_recv, own_sem, lane_send, lane_recv, plane_send, plane_recv,
        load_sem, matrix_send, matrix_recv, out_sem, in_sem, row_send, row_recv,
        near_send, near_recv, far_send, far_recv,
    ) = refs
    n = lay.n_tp
    rows, width = skip_ref.shape
    length, breadth = read_ref.shape
    pairs = breadth // PAIR
    span = range(pairs)
    last = lay.planes - 1
    spot, me = lax.axis_index("sp"), lax.axis_index("tp")
    z, y = spot // lay.lanes, lax.rem(spot, lay.lanes)
    x, c = me // lay.cores, lax.rem(me, lay.cores)
    beside = [z * lay.lanes + lax.rem(y + s, lay.lanes) for s in range(1, lay.lanes)]
    line = [lax.rem(spot + s * lay.lanes, lay.n_sp) for s in range(1, lay.planes)]
    peers = [lax.rem(me + s, n) for s in range(1, n)]
    partners = [x * lay.cores + lax.rem(c + j, lay.cores) for j in range(1, lay.cores)]
    remote = [lax.rem(x + i, lay.sides) * lay.cores + c for i in range(1, lay.sides)]

    barrier = pltpu.get_barrier_semaphore()
    for axis, others in (("sp", beside + line), ("tp", peers)):
        for other in others:
            pl.semaphore_signal(barrier, inc=1, **to(**{axis: other}))
    pl.semaphore_wait(barrier, len(beside) + len(line) + len(peers))

    relay = Relay(lay, (gate_ref, up_ref, down_ref), whole, relay_send, relay_recv, own_sem)
    for m in (GATE, UP):
        relay.forward(m, 0) if last else None
        relay.cross(m, 0)
    for m in (GATE, UP, DOWN):
        relay.own(m).start()

    def place_matrix(i, j):
        side, core = lax.rem(x + lay.sides - i, lay.sides), lax.rem(c + lay.cores - j, lay.cores)
        return side * lay.cores + core

    def pass_matrix(i, j):
        source = matrix_ref if i == 0 or j == 0 else matrix.at[i, 0]
        target = partners[j - 1] if j else remote[i - 1]
        return pltpu.make_async_remote_copy(
            src_ref=source,
            dst_ref=matrix.at[i, j],
            send_sem=matrix_send.at[i, j],
            recv_sem=matrix_recv.at[i, j],
            **to(tp=target),
        )

    own_matrix = pltpu.make_async_copy(matrix_ref, matrix.at[0, 0], load_sem)
    own_matrix.start()
    for i in range(1, lay.sides):
        pass_matrix(i, 0).start()
    for j in range(1, lay.cores):
        pass_matrix(0, j).start()

    diagonal = jnp.where(
        lax.broadcasted_iota(jnp.int32, (PAIR, PAIR), 0)
        == lax.broadcasted_iota(jnp.int32, (PAIR, PAIR), 1),
        1.0,
        0.0,
    )
    for p in span:
        memory[p, :PAIR] = jnp.zeros((PAIR, PAIR), f32)
        memory[p, PAIR:] = diagonal

    chunks = length // CHUNK

    def one(turn, _):
        if last:

            @pl.when(turn == chunks // 3)
            def _():
                relay.take(GATE, 1)
                if last > 1:
                    relay.forward(GATE, 1)
                for lane in range(1, lay.lanes):
                    relay.start(relay.aside(GATE, 1, lane))

            @pl.when(turn == 2 * chunks // 3)
            def _():
                relay.take(UP, 1)

        here = pl.ds(pl.multiple_of(turn * CHUNK, CHUNK), CHUNK)
        advance_chunk(
            here, read_ref, key_ref, value_ref, forget_ref, added_ref, rate_ref, forget_off_ref,
            rate_off_ref, local_ref, coef_ref, memory,
        )
        return 0

    lax.fori_loop(0, chunks, one, 0)

    for p in span:
        lane_ref[y, 0, p] = fold(memory[p, :PAIR]).astype(bf16)
        lane_ref[y, 1, p] = fold(memory[p, PAIR:]).astype(bf16)
    lane_copies = [
        pltpu.make_async_remote_copy(
            src_ref=lane_ref.at[y],
            dst_ref=lane_ref.at[y],
            send_sem=lane_send.at[s],
            recv_sem=lane_recv.at[s],
            **to(sp=other),
        )
        for s, other in enumerate(beside)
    ]
    for copy in lane_copies:
        copy.start()
    if last:
        for lane in range(1, lay.lanes):
            relay.start(relay.aside(GATE, -1, lane))
        relay.cross(UP, 1)
    for copy in lane_copies:
        copy.wait_recv()
    state = [stack(lane_ref[0, 0, p].astype(f32)) for p in span]
    move = [stack(lane_ref[0, 1, p].astype(f32)) for p in span]
    own_state = [jnp.where(y > 0, state[p], 0.0) for p in span]
    own_move = [jnp.where(y > 0, move[p], diagonal) for p in span]
    for t in range(1, lay.lanes):
        for p in span:
            step = stack(lane_ref[t, 1, p].astype(f32))
            state[p] = chain(state[p], step) + stack(lane_ref[t, 0, p].astype(f32))
            move[p] = chain(move[p], step)
            if t < lay.lanes - 1:
                own_state[p] = jnp.where(y > t, state[p], own_state[p])
                own_move[p] = jnp.where(y > t, move[p], own_move[p])
    for p in span:
        mine_ref[0, p] = fold(state[p]).astype(bf16)
        mine_ref[1, p] = fold(move[p]).astype(bf16)

    def onward(s):
        return pltpu.make_async_remote_copy(
            src_ref=mine_ref,
            dst_ref=plane_ref.at[s - 1],
            send_sem=plane_send.at[s - 1],
            recv_sem=plane_recv.at[s - 1],
            **to(sp=line[s - 1]),
        )

    for s in range(1, lay.planes):
        pl.when(z + s < lay.planes)(onward(s).start)
    if last > 1:
        relay.forward(UP, 1)
        relay.take(GATE, 2)
        if last > 2:
            relay.forward(GATE, 2)
        relay.cross(GATE, 2)
    for p in span:
        carried_ref[p] = jnp.zeros((PAIR, PAIR), f32)
    for s in range(last, 0, -1):

        @pl.when(z >= s)
        def _(s=s):
            onward(s).wait_recv()
            for p in span:
                carried_ref[p] = chain(
                    carried_ref[p], stack(plane_ref[s - 1, 1, p].astype(f32))
                ) + stack(plane_ref[s - 1, 0, p].astype(f32))

    for p in span:
        carried_ref[p] = chain(carried_ref[p], own_move[p]) + own_state[p]

    for i in range(1, lay.sides):
        pass_matrix(i, 0).wait_recv()
        for j in range(1, lay.cores):
            pass_matrix(i, j).start()

    def send(s):
        return pltpu.make_async_remote_copy(
            src_ref=mixed.at[s],
            dst_ref=gathered.at[s],
            send_sem=out_sem.at[s],
            recv_sem=in_sem.at[s],
            **to(tp=peers[s]),
        )

    for s in range(n):
        target = peers[s] if s < n - 1 else me
        here = pl.ds(pl.multiple_of(target * rows, rows), rows)
        for p in span:
            at = slice(p * PAIR, (p + 1) * PAIR)
            outcome = local_ref[here, at] + mm(coef_ref[here, at].astype(f32), carried_ref[p], NT, 1)
            centred = outcome - head_sums(outcome) * (1.0 / PER_GROUP_DIMS)
            spread = head_sums(centred * centred) * (1.0 / PER_GROUP_DIMS)
            normed = centred * lax.rsqrt(spread + group_eps)
            reward = head_sums(
                read_ref[here, at].astype(f32) * key_ref[here, at].astype(f32) * scales_ref[:, at]
            )
            block = (
                (normed + reward * value_ref[here, at].astype(f32))
                * switch_ref[here, at].astype(f32)
            ).astype(bf16)
            if s < n - 1:
                mixed[s, :, at] = block
            else:
                gathered[s, :, at] = block
        if s < n - 1:
            send(s).start()
    if last > 1:
        relay.take(UP, 2)
        if last > 2:
            relay.forward(UP, 2)
        relay.cross(UP, 2)
    for s in range(n - 1):
        send(s).wait_recv()
    own_matrix.wait()
    for i in range(lay.sides):
        for j in range(1, lay.cores):
            pass_matrix(i, j).wait_recv()
    total = jnp.zeros((rows, width), f32)
    for i in range(lay.sides):
        for j in range(lay.cores):
            slot = lax.rem(me - place_matrix(i, j) + 2 * n - 1, n)
            total += jnp.dot(gathered[slot], matrix[i, j], preferred_element_type=f32)
    stream = skip_ref[...].astype(f32) + total.astype(bf16).astype(f32)
    stream_ref[...] = stream
    scale = lax.rsqrt(jnp.mean(stream * stream, axis=-1, keepdims=True) + norm_eps)
    mine = pl.ds(pl.multiple_of(me * rows, rows), rows)
    rows_ref[mine] = (stream * scale * gain_ref[...]).astype(bf16)

    def pass_rows(source, target, slot):
        piece = rows_ref.at[pl.ds(pl.multiple_of(source * rows, rows), rows)]
        return pltpu.make_async_remote_copy(
            src_ref=piece,
            dst_ref=piece,
            send_sem=row_send.at[slot],
            recv_sem=row_recv.at[slot],
            **to(tp=target),
        )

    row_copies = []
    for i in range(1, lay.sides):
        copy = pass_rows(me, remote[i - 1], i * lay.cores)
        copy.start()
        row_copies.append(copy)
    for i in range(lay.sides):
        source = lax.rem(x + lay.sides - i, lay.sides) * lay.cores + c
        if i:
            row_copies[i - 1].wait_recv()
        for j in range(1, lay.cores):
            copy = pass_rows(source, partners[j - 1], i * lay.cores + j)
            copy.start()
            row_copies.append(copy)
    for r in range(3, last + 1):
        for m in (GATE, UP):
            relay.take(m, r)
            if r < last:
                relay.forward(m, r)
            relay.cross(m, r)
    if last:
        relay.forward(DOWN, 0)
    relay.cross(DOWN, 0)
    for copy in row_copies[lay.sides - 1 :]:
        copy.wait_recv()

    for m in (GATE, UP):
        relay.own(m).wait()
        for lane in range(1, lay.lanes):
            for hop in range(-last, last + 1):
                relay.arrive(m, hop, lane)

    def down_step(r):
        if r <= last:
            relay.take(DOWN, r)
            if r < last:
                relay.forward(DOWN, r)
            relay.cross(DOWN, r)

    down_step(1)
    units = hidden_ref.shape[1]
    tile = 256 if units % 256 == 0 else 128 if units % 128 == 0 else units
    for first in range(0, units, tile):
        columns = slice(first, first + tile)
        gated = jnp.dot(rows_ref[...], whole[GATE, :, columns], preferred_element_type=f32)
        raised = jnp.dot(rows_ref[...], whole[UP, :, columns], preferred_element_type=f32)
        hidden_ref[:, columns] = (gated * jax.nn.sigmoid(gated) * raised).astype(bf16)

    relay.own(DOWN).wait()
    part = width // lay.planes
    order = list(range(1, lay.sides)) + [0]
    hops = [0] + [way * r for r in range(1, last + 1) for way in (1, -1)]

    def within(t, i, j):
        return pltpu.make_async_remote_copy(
            src_ref=inner.at[t, j - 1, i],
            dst_ref=near.at[t, j - 1, i],
            send_sem=near_send.at[t, i, j - 1],
            recv_sem=near_recv.at[t, i, j - 1],
            **to(tp=partners[j - 1]),
        )

    def between(t, i):
        return pltpu.make_async_remote_copy(
            src_ref=outer.at[t, i - 1],
            dst_ref=far.at[t, i - 1],
            send_sem=far_send.at[t, i - 1],
            recv_sem=far_recv.at[t, i - 1],
            **to(tp=remote[i - 1]),
        )

    def product(weight, i, j):
        target = lax.rem(x + i, lay.sides) * lay.cores + lax.rem(c + j, lay.cores)
        piece = hidden_ref[pl.ds(pl.multiple_of(target * rows, rows), rows)]
        return lax.dot_general(piece, weight, NT, preferred_element_type=f32)

    for t, hop in enumerate(hops):
        if hop >= 0:
            down_step(hop + 2)
        for lane in range(1, lay.lanes):
            relay.arrive(DOWN, hop, lane)

        @pl.when(relay.held(hop))
        def _(t=t, hop=hop):
            weight = whole[DOWN, pl.ds(pl.multiple_of((z - hop) * part, part), part)]
            for i in order:
                for j in range(1, lay.cores):
                    inner[t, j - 1, i] = product(weight, i, j).astype(bf16)
                    within(t, i, j).start()
            for i in order:
                own[t, i] = product(weight, i, 0)
            for i in order:
                sums = own[t, i]
                for j in range(1, lay.cores):
                    within(t, i, j).wait_recv()
                    sums += near[t, j - 1, i].astype(f32)
                if i:
                    outer[t, i - 1] = sums.astype(bf16)
                    between(t, i).start()
                else:
                    own[t, 0] = sums

    for t, hop in enumerate(hops):

        @pl.when(relay.held(hop))
        def _(t=t, hop=hop):
            columns = pl.ds(pl.multiple_of((z - hop) * part, part), part)
            sums = own[t, 0]
            for i in range(1, lay.sides):
                between(t, i).wait_recv()
                sums += far[t, i - 1].astype(f32)
            sums = sums.astype(bf16).astype(f32)
            out_ref[:, columns] = (stream_ref[:, columns] + half_step * sums).astype(bf16)

    for m in (GATE, UP, DOWN):
        relay.settle(m)
    for copy in lane_copies + row_copies:
        copy.wait_send()
    for s in range(1, lay.planes):
        pl.when(z + s < lay.planes)(onward(s).wait_send)
    for i in range(lay.sides):
        for j in range(lay.cores):
            if i or j:
                pass_matrix(i, j).wait_send()
    for s in range(n - 1):
        send(s).wait_send()
    for t, hop in enumerate(hops):

        @pl.when(relay.held(hop))
        def _(t=t):
            for i in order:
                for j in range(1, lay.cores):
                    within(t, i, j).wait_send()
                if i:
                    between(t, i).wait_send()


def per_device(
    lay,
    skip_stream,
    acceptance_signal,
    lookup_mapped,
    payload_mapped,
    result_switch,
    forget_dynamic_share,
    additive_forget_logarithm,
    forget_feature_offset,
    substitution_dynamic_share,
    substitution_feature_offset,
    diagonal_reward_scales,
    result_matrix,
    mlp_rescaler,
    switch_matrix,
    expand_matrix,
    contract_matrix,
):
    rows, width = skip_stream.shape
    length, breadth = acceptance_signal.shape
    depth, units = switch_matrix.shape
    pairs = breadth // PAIR
    n = lay.n_tp
    one = (2, pairs, PER_GROUP_DIMS, PAIR)
    lanes, planes = max(lay.lanes - 1, 1), max(lay.planes - 1, 1)
    cores, sides = max(lay.cores - 1, 1), max(lay.sides - 1, 1)
    places = (2 * lay.planes - 1) * lay.lanes
    hops = 2 * lay.planes - 1
    part = width // lay.planes
    dma = pltpu.SemaphoreType.DMA
    vmem, anywhere = pl.BlockSpec(memory_space=pltpu.VMEM), pl.BlockSpec(memory_space=pl.ANY)
    return pl.pallas_call(
        functools.partial(layer_kernel, lay, hops),
        in_specs=[vmem] * 11 + [anywhere, vmem] + [anywhere] * 3,
        out_specs=vmem,
        out_shape=jax.ShapeDtypeStruct((rows, width), bf16),
        scratch_shapes=[
            pltpu.VMEM((length, breadth), f32),
            pltpu.VMEM((length, breadth), bf16),
            pltpu.VMEM((pairs, 2 * PAIR, PAIR), f32),
            pltpu.VMEM((lay.lanes,) + one, bf16),
            pltpu.VMEM((planes,) + one, bf16),
            pltpu.VMEM(one, bf16),
            pltpu.VMEM((pairs, PAIR, PAIR), f32),
            pltpu.VMEM((n - 1, rows, breadth), bf16),
            pltpu.VMEM((n, rows, breadth), bf16),
            pltpu.VMEM((lay.sides, lay.cores, breadth, width), bf16),
            pltpu.VMEM((rows, width), f32),
            pltpu.VMEM((length, width), bf16),
            pltpu.VMEM((length, units), bf16),
            pltpu.VMEM((3, width, units), bf16),
            pltpu.VMEM((hops, lay.sides, rows, part), f32),
            pltpu.VMEM((hops, cores, lay.sides, rows, part), bf16),
            pltpu.VMEM((hops, cores, lay.sides, rows, part), bf16),
            pltpu.VMEM((hops, sides, rows, part), bf16),
            pltpu.VMEM((hops, sides, rows, part), bf16),
            dma((3, places)),
            dma((3, places)),
            dma((3,)),
            dma((lanes,)),
            dma((lanes,)),
            dma((planes,)),
            dma((planes,)),
            dma,
            dma((lay.sides, lay.cores)),
            dma((lay.sides, lay.cores)),
            dma((n,)),
            dma((n,)),
            dma((n,)),
            dma((n,)),
            dma((hops, lay.sides, cores)),
            dma((hops, lay.sides, cores)),
            dma((hops, sides)),
            dma((hops, sides)),
        ],
        compiler_params=pltpu.CompilerParams(
            collective_id=0, has_side_effects=True, vmem_limit_bytes=63 * 2**20
        ),
        cost_estimate=pl.CostEstimate(
            flops=6 * length * width * units, bytes_accessed=6 * width * units, transcendentals=0
        ),
        name="layer",
    )(
        skip_stream,
        acceptance_signal,
        lookup_mapped,
        payload_mapped,
        result_switch,
        forget_dynamic_share,
        additive_forget_logarithm,
        forget_feature_offset[None, :],
        substitution_dynamic_share,
        substitution_feature_offset[None, :],
        diagonal_reward_scales[None, :],
        result_matrix,
        mlp_rescaler[None, :],
        switch_matrix,
        expand_matrix,
        contract_matrix,
    )


def solution(mesh):
    placed = (
        P(("sp", "tp"), None),
        P("sp", "tp"),
        P("sp", "tp"),
        P("sp", "tp"),
        P("sp", "tp"),
        P("sp", "tp"),
        P("sp", "tp"),
        P("tp"),
        P("sp", "tp"),
        P("tp"),
        P("tp"),
        P("tp", None),
        P(),
        P("sp", "tp"),
        P("sp", "tp"),
        P("sp", "tp"),
    )
    return jax.shard_map(
        functools.partial(per_device, Layout(mesh)),
        mesh=mesh,
        in_specs=placed,
        out_specs=P(("sp", "tp"), None),
        check_vma=False,
    )
```

```python
import functools

import jax
import jax.numpy as jnp
from jax import lax
from jax.experimental import pallas as pl
from jax.experimental.pallas import tpu as pltpu
from jax.sharding import PartitionSpec as P

PER_GROUP_DIMS = 64


norm_eps = 1e-06
group_eps = 0.00064
half_step = 0.5
exact = lax.Precision.HIGHEST

PAIR = 2 * PER_GROUP_DIMS
CHUNK = 64
ROWS_OUT = 256
NT = (((1,), (1,)), ((), ()))
NN = (((1,), (0,)), ((), ()))
TN = (((0,), (0,)), ((), ()))
bf16 = jnp.bfloat16
f32 = jnp.float32
P_SCORE, P_INV, P_SOLVE, P_OUT, P_STATE = 3, 1, 3, 3, 1


def mm(left, right, dims, passes):
    if passes == 6:
        return lax.dot_general(left, right, dims, precision=exact, preferred_element_type=f32)
    left_hi, right_hi = left.astype(bf16), right.astype(bf16)
    total = lax.dot_general(left_hi, right_hi, dims, preferred_element_type=f32)
    if passes == 3:
        left_lo = (left - left_hi.astype(f32)).astype(bf16)
        right_lo = (right - right_hi.astype(f32)).astype(bf16)
        total += lax.dot_general(left_hi, right_lo, dims, preferred_element_type=f32)
        total += lax.dot_general(left_lo, right_hi, dims, preferred_element_type=f32)
    return total


def halves(shape):
    return lax.broadcasted_iota(jnp.int32, shape, 1) < PER_GROUP_DIMS


def stack(values):
    first = halves(values.shape)
    zero = jnp.zeros_like(values)
    return jnp.concatenate([jnp.where(first, values, zero), jnp.where(first, zero, values)], 0)


def fold(values):
    size = values.shape[0] // 2
    return values[:size] + values[size:]


def head_sums(values):
    row = lax.broadcasted_iota(jnp.int32, (PAIR, PAIR), 0) // PER_GROUP_DIMS
    col = lax.broadcasted_iota(jnp.int32, (PAIR, PAIR), 1) // PER_GROUP_DIMS
    ones = jnp.where(row == col, 1.0, 0.0).astype(bf16)
    hi = values.astype(bf16)
    left = values - hi.astype(f32)
    mid = left.astype(bf16)
    low = (left - mid.astype(f32)).astype(bf16)
    return (
        jnp.dot(hi, ones, preferred_element_type=f32)
        + jnp.dot(mid, ones, preferred_element_type=f32)
        + jnp.dot(low, ones, preferred_element_type=f32)
    )


def advance_chunk(
    here, read_ref, key_ref, value_ref, forget_ref, added_ref, rate_ref, forget_off_ref,
    rate_off_ref, local_ref, coef_ref, memory,
):
    pairs = read_ref.shape[1] // PAIR
    span = range(pairs)
    row = lax.broadcasted_iota(jnp.int32, (PAIR, PAIR), 0)
    col = lax.broadcasted_iota(jnp.int32, (PAIR, PAIR), 1)
    diagonal = jnp.where(row == col, 1.0, 0.0)
    same_head = (row // CHUNK) == (col // CHUNK)
    strict = same_head & (col < row)
    inclusive = same_head & (col <= row)

    lower = (
        lax.broadcasted_iota(jnp.int32, (CHUNK, CHUNK), 1)
        <= lax.broadcasted_iota(jnp.int32, (CHUNK, CHUNK), 0)
    )
    lower = jnp.where(lower, 1.0, 0.0)
    first = halves((CHUNK, PAIR))
    at = [slice(p * PAIR, (p + 1) * PAIR) for p in span]
    decay_rate = [
        jax.nn.sigmoid(forget_off_ref[:, at[p]] + forget_ref[here, at[p]].astype(f32)) for p in span
    ]
    log_step = [
        -0.6065306597126334 * decay_rate[p]
        + jnp.where(first, added_ref[here, 2 * p : 2 * p + 1], added_ref[here, 2 * p + 1 : 2 * p + 2])
        for p in span
    ]
    cumulate = [mm(lower, log_step[p], NN, 6) for p in span]
    key = [key_ref[here, at[p]].astype(f32) for p in span]
    unit = [key[p] * lax.rsqrt(head_sums(key[p] * key[p]) + norm_eps) for p in span]
    erase = [
        unit[p] * jax.nn.sigmoid(rate_off_ref[:, at[p]] + rate_ref[here, at[p]].astype(f32))
        for p in span
    ]
    middle = [cumulate[p][CHUNK // 2 - 1 : CHUNK // 2] for p in span]
    last = [cumulate[p][CHUNK - 1 : CHUNK] for p in span]
    growth = [jnp.exp(cumulate[p] - middle[p]) for p in span]
    shrink = [jnp.exp(middle[p] - cumulate[p]) for p in span]
    to_middle = [jnp.exp(middle[p]) for p in span]
    from_middle = [jnp.exp(last[p] - middle[p]) for p in span]
    over_chunk = [jnp.exp(last[p]) for p in span]
    before = [jnp.exp(cumulate[p] - log_step[p] - middle[p]) * unit[p] for p in span]
    read = [read_ref[here, at[p]].astype(f32) * growth[p] for p in span]
    key_back = [key[p] * shrink[p] for p in span]
    erase_back = [erase[p] * shrink[p] for p in span]
    score = [
        mm(
            jnp.concatenate([stack(before[p]), stack(read[p])], 0),
            jnp.concatenate([stack(key_back[p]), stack(erase_back[p])], 0),
            NT,
            P_SCORE,
        )
        for p in span
    ]
    key_past = [jnp.where(strict, score[p][:PAIR, :PAIR], 0.0) for p in span]
    erase_past = [jnp.where(strict, score[p][:PAIR, PAIR:], 0.0) for p in span]
    key_read = [jnp.where(inclusive, score[p][PAIR:, :PAIR], 0.0) for p in span]
    erase_read = [jnp.where(inclusive, score[p][PAIR:, PAIR:], 0.0) for p in span]
    value = [stack(value_ref[here, at[p]]).astype(f32) for p in span]
    recall = [mm(key_past[p], value[p], NN, P_SOLVE) for p in span]
    inverse = [
        diagonal - jnp.where((row // 2) == (col // 2), erase_past[p], 0.0) for p in span
    ]
    size = 2
    while size < CHUNK:
        off = ((row // (2 * size)) == (col // (2 * size))) & ((row // size) != (col // size))
        part = [mm(jnp.where(off, erase_past[p], 0.0), inverse[p], NN, P_INV) for p in span]
        inverse = [inverse[p] - mm(inverse[p], part[p], NN, P_INV) for p in span]
        size *= 2
    solved = [
        mm(
            inverse[p],
            jnp.concatenate([recall[p], stack(before[p] * to_middle[p])], 1),
            NN,
            P_SOLVE,
        )
        for p in span
    ]
    inner = [
        mm(
            jnp.concatenate([key_read[p], -erase_read[p]], 1),
            jnp.concatenate(
                [jnp.concatenate([value[p], jnp.zeros_like(value[p])], 1), solved[p]], 0
            ),
            NN,
            P_OUT,
        )
        for p in span
    ]
    local = [fold(inner[p][:, :PAIR]) for p in span]
    from_start = [fold(inner[p][:, PAIR:]) + read[p] * to_middle[p] for p in span]
    both = [memory[p] for p in span]
    passed = [mm(from_start[p], both[p], NT, P_STATE) for p in span]
    for p in span:
        local_ref[here, at[p]] = local[p] + passed[p][:, :PAIR]
        coef_ref[here, at[p]] = passed[p][:, PAIR:].astype(bf16)
    key_end = [key_back[p] * from_middle[p] for p in span]
    erase_end = [erase_back[p] * from_middle[p] for p in span]
    recalled = [fold(solved[p][:, :PAIR]) for p in span]
    carried_map = [fold(solved[p][:, PAIR:]) for p in span]
    added = [
        mm(
            jnp.concatenate([value_ref[here, at[p]].astype(f32), -recalled[p]], 0),
            jnp.concatenate([key_end[p], erase_end[p]], 0),
            TN,
            P_OUT,
        )
        for p in span
    ]
    step_map = [mm(carried_map[p], erase_end[p], TN, P_OUT) for p in span]
    for p in span:
        moved = mm(both[p], jnp.where(same_head, step_map[p], 0.0), NN, P_STATE)
        kept = both[p] * over_chunk[p] - moved
        memory[p, :PAIR] = kept[:PAIR] + jnp.where(same_head, added[p], 0.0)
        memory[p, PAIR:] = kept[PAIR:]


class Layout:
    def __init__(self, mesh):
        self.n_sp, self.n_tp = mesh.shape["sp"], mesh.shape["tp"]
        devices = list(mesh.devices.flat)
        spots = [getattr(d, "coords", None) for d in devices]
        self.lanes = self.cores = 1
        if all(s is not None for s in spots):
            self.lanes = len({s[1] for s in spots})
            self.cores = len({getattr(d, "core_on_chip", 0) for d in devices})
        if self.n_sp % self.lanes:
            self.lanes = 1
        if self.n_tp % self.cores:
            self.cores = 1
        self.planes, self.sides = self.n_sp // self.lanes, self.n_tp // self.cores


def to(**where):
    return dict(device_id=where, device_id_type=pl.DeviceIdType.MESH)


def chain(total, step):
    return mm(total, step, NN, 1) + mm(total - total.astype(bf16).astype(f32), step, NN, 1)


GATE, UP, DOWN = range(3)
WIDE = (UP,)


class Relay:
    def __init__(self, lay, blocks, whole, send_sem, recv_sem, own_sem):
        self.lay, self.blocks, self.whole, self.own_sem = lay, blocks, whole, own_sem
        self.send_sem, self.recv_sem = send_sem, recv_sem
        me = lax.axis_index("sp")
        self.z, self.y = me // lay.lanes, lax.rem(me, lay.lanes)
        self.depth = blocks[0].shape[0]

    def slot(self, hop, lane):
        return (hop + self.lay.planes - 1) * self.lay.lanes + lane

    def held(self, hop):
        return (self.z >= hop) & (self.z < self.lay.planes + hop)

    def wide(self, matrix, hop):
        if matrix not in WIDE:
            return False
        first, last = self.z == hop, self.z == self.lay.planes - 1 + hop
        return first | last if hop == 0 else first if hop > 0 else last

    def part(self, matrix, hop, lane):
        source = (self.z - hop) * self.lay.lanes + lax.rem(
            self.y + self.lay.lanes - lane, self.lay.lanes
        )
        first = pl.multiple_of(source * self.depth, self.depth)
        return self.whole.at[matrix, pl.ds(first, self.depth)]

    def copy(self, matrix, source, place, plane, lane):
        return pltpu.make_async_remote_copy(
            src_ref=self.blocks[matrix] if source == (0, 0) else self.part(matrix, *source),
            dst_ref=self.part(matrix, *source),
            send_sem=self.send_sem.at[matrix, self.slot(*place)],
            recv_sem=self.recv_sem.at[matrix, self.slot(*place)],
            **to(sp=plane * self.lay.lanes + lane),
        )

    def ahead(self, matrix, hop, way, lane=0):
        there = self.z + way
        wanted = self.held(hop) & (there >= 0) & (there < self.lay.planes)
        if lane:
            wanted = wanted & self.wide(matrix, hop)
        return self.copy(matrix, (hop, lane), (hop + way, lane), there, self.y), wanted

    def aside(self, matrix, hop, lane):
        beside = lax.rem(self.y + lane, self.lay.lanes)
        wanted = self.held(hop)
        if hop and matrix in WIDE:
            wanted = wanted & ~self.wide(matrix, hop)
        return self.copy(matrix, (hop, 0), (hop, lane), self.z, beside), wanted

    def start(self, pair):
        pl.when(pair[1])(pair[0].start)

    def own(self, matrix):
        return pltpu.make_async_copy(
            self.blocks[matrix], self.part(matrix, 0, 0), self.own_sem.at[matrix]
        )

    def arrive(self, matrix, hop, lane, wide=None):
        piece = self.part(matrix, hop, lane)
        slot = self.slot(hop, lane)
        wait = pltpu.make_async_remote_copy(
            src_ref=piece,
            dst_ref=piece,
            send_sem=self.send_sem.at[matrix, slot],
            recv_sem=self.recv_sem.at[matrix, slot],
            **to(sp=lax.axis_index("sp")),
        ).wait_recv
        wanted = self.held(hop)
        if wide is not None and matrix in WIDE:
            wanted = wanted & (self.wide(matrix, hop) if wide else ~self.wide(matrix, hop))
        pl.when(wanted)(wait)

    def take(self, matrix, reach):
        for hop in (reach, -reach):
            self.arrive(matrix, hop, 0)

    def forward(self, matrix, reach):
        for way in (1, -1):
            self.start(self.ahead(matrix, way * reach, way))

    def take_wide(self, matrix, reach):
        for hop in (reach, -reach):
            for lane in range(1, self.lay.lanes):
                self.arrive(matrix, hop, lane, wide=True)

    def forward_wide(self, matrix, reach):
        for way in (1, -1):
            for lane in range(1, self.lay.lanes):
                self.start(self.ahead(matrix, way * reach, way, lane))

    def cross(self, matrix, reach):
        for hop in (reach, -reach) if reach else (0,):
            for lane in range(1, self.lay.lanes):
                self.start(self.aside(matrix, hop, lane))

    def settle(self, matrix):
        last = self.lay.planes - 1
        for reach in range(last + 1):
            for way in (1, -1):
                if reach < last:
                    for lane in range(self.lay.lanes if matrix in WIDE else 1):
                        copy, wanted = self.ahead(matrix, way * reach, way, lane)
                        pl.when(wanted)(copy.wait_send)
            for hop in (reach, -reach) if reach else (0,):
                for lane in range(1, self.lay.lanes):
                    copy, wanted = self.aside(matrix, hop, lane)
                    pl.when(wanted)(copy.wait_send)


def layer_kernel(lay, steps, *refs):
    forget_off_ref, rate_off_ref, scales_ref, gain_ref, *given = refs[:16]
    given, (matrix_ref, gate_ref, up_ref, down_ref) = given[:8], given[8:12]
    out_ref = refs[16]
    loaded = refs[17:25]
    read_ref, key_ref, value_ref, forget_ref, added_ref, rate_ref, switch_ref, skip_ref = loaded
    (
        input_sem,
        local_ref, coef_ref, memory, lane_ref, plane_ref, mine_ref, carried_ref, mixed, gathered,
        matrix, stream_ref, rows_ref, hidden_ref, whole, own, inner, near, outer, far,
        relay_send, relay_recv, own_sem, lane_send, lane_recv, plane_send, plane_recv,
        load_sem, matrix_send, matrix_recv, out_sem, in_sem, row_send, row_recv,
        near_send, near_recv, far_send, far_recv,
    ) = refs[25:]
    n = lay.n_tp
    rows, width = skip_ref.shape
    length, breadth = read_ref.shape
    pairs = breadth // PAIR
    span = range(pairs)
    last = lay.planes - 1
    spot, me = lax.axis_index("sp"), lax.axis_index("tp")
    z, y = spot // lay.lanes, lax.rem(spot, lay.lanes)
    x, c = me // lay.cores, lax.rem(me, lay.cores)
    beside = [z * lay.lanes + lax.rem(y + s, lay.lanes) for s in range(1, lay.lanes)]
    line = [lax.rem(spot + s * lay.lanes, lay.n_sp) for s in range(1, lay.planes)]
    peers = [lax.rem(me + s, n) for s in range(1, n)]
    partners = [x * lay.cores + lax.rem(c + j, lay.cores) for j in range(1, lay.cores)]
    remote = [lax.rem(x + i, lay.sides) * lay.cores + c for i in range(1, lay.sides)]

    barrier = pltpu.get_barrier_semaphore()
    for axis, others in (("sp", beside + line), ("tp", peers)):
        for other in others:
            pl.semaphore_signal(barrier, inc=1, **to(**{axis: other}))
    pl.semaphore_wait(barrier, len(beside) + len(line) + len(peers))

    relay = Relay(lay, (gate_ref, up_ref, down_ref), whole, relay_send, relay_recv, own_sem)
    for m in (GATE, UP):
        relay.forward(m, 0) if last else None
        relay.cross(m, 0)

    def place_matrix(i, j):
        side, core = lax.rem(x + lay.sides - i, lay.sides), lax.rem(c + lay.cores - j, lay.cores)
        return side * lay.cores + core

    def pass_matrix(i, j):
        source = matrix_ref if i == 0 or j == 0 else matrix.at[i, 0]
        target = partners[j - 1] if j else remote[i - 1]
        return pltpu.make_async_remote_copy(
            src_ref=source,
            dst_ref=matrix.at[i, j],
            send_sem=matrix_send.at[i, j],
            recv_sem=matrix_recv.at[i, j],
            **to(tp=target),
        )

    inputs = [
        pltpu.make_async_copy(given[k], loaded[k], input_sem.at[k]) for k in range(len(given))
    ]
    for copy in inputs:
        copy.start()
    own_matrix = pltpu.make_async_copy(matrix_ref, matrix.at[0, 0], load_sem)
    own_matrix.start()
    for i in range(1, lay.sides):
        pass_matrix(i, 0).start()
    for j in range(1, lay.cores):
        pass_matrix(0, j).start()

    for m in (GATE, UP, DOWN):
        relay.own(m).start()
    diagonal = jnp.where(
        lax.broadcasted_iota(jnp.int32, (PAIR, PAIR), 0)
        == lax.broadcasted_iota(jnp.int32, (PAIR, PAIR), 1),
        1.0,
        0.0,
    )
    for p in span:
        memory[p, :PAIR] = jnp.zeros((PAIR, PAIR), f32)
        memory[p, PAIR:] = diagonal

    chunks = length // CHUNK
    for copy in inputs[:6]:
        copy.wait()

    def gate_aside(first):
        for lane in range(1, lay.lanes):
            for hop, wanted in ((1, z > 0), (-1, z == 0)) if first else ((-1, z > 0),):
                copy, held = relay.aside(GATE, hop, lane)
                relay.start((copy, held & wanted))

    def one(turn, _):
        if last:

            @pl.when(turn == 5 * chunks // 12)
            def _():
                relay.take(GATE, 1)
                if last > 1:
                    relay.forward(GATE, 1)
                gate_aside(True)

            @pl.when(turn == 10 * chunks // 12)
            def _():
                relay.take(UP, 1)
                if last > 1:
                    relay.forward(UP, 1)
                for lane in range(1, lay.lanes):
                    relay.arrive(UP, 0, lane)
                relay.forward_wide(UP, 0)

        here = pl.ds(pl.multiple_of(turn * CHUNK, CHUNK), CHUNK)
        advance_chunk(
            here, read_ref, key_ref, value_ref, forget_ref, added_ref, rate_ref, forget_off_ref,
            rate_off_ref, local_ref, coef_ref, memory,
        )
        return 0

    lax.fori_loop(0, chunks, one, 0)

    for p in span:
        lane_ref[y, 0, p] = fold(memory[p, :PAIR]).astype(bf16)
        lane_ref[y, 1, p] = fold(memory[p, PAIR:]).astype(bf16)
    lane_copies = [
        pltpu.make_async_remote_copy(
            src_ref=lane_ref.at[y],
            dst_ref=lane_ref.at[y],
            send_sem=lane_send.at[s],
            recv_sem=lane_recv.at[s],
            **to(sp=other),
        )
        for s, other in enumerate(beside)
    ]
    for copy in lane_copies:
        copy.start()
    if last:
        gate_aside(False)
        relay.cross(UP, 1)
    for copy in lane_copies:
        copy.wait_recv()
    state = [stack(lane_ref[0, 0, p].astype(f32)) for p in span]
    move = [stack(lane_ref[0, 1, p].astype(f32)) for p in span]
    own_state = [jnp.where(y > 0, state[p], 0.0) for p in span]
    own_move = [jnp.where(y > 0, move[p], diagonal) for p in span]
    for t in range(1, lay.lanes):
        for p in span:
            step = stack(lane_ref[t, 1, p].astype(f32))
            state[p] = chain(state[p], step) + stack(lane_ref[t, 0, p].astype(f32))
            move[p] = chain(move[p], step)
            if t < lay.lanes - 1:
                own_state[p] = jnp.where(y > t, state[p], own_state[p])
                own_move[p] = jnp.where(y > t, move[p], own_move[p])
    for p in span:
        mine_ref[0, p] = fold(state[p]).astype(bf16)
        mine_ref[1, p] = fold(move[p]).astype(bf16)

    def onward(s):
        return pltpu.make_async_remote_copy(
            src_ref=mine_ref,
            dst_ref=plane_ref.at[s - 1],
            send_sem=plane_send.at[s - 1],
            recv_sem=plane_recv.at[s - 1],
            **to(sp=line[s - 1]),
        )

    for s in range(1, lay.planes):
        pl.when(z + s < lay.planes)(onward(s).start)
    if last > 1:
        for m in (GATE, UP):
            relay.take(m, 2)
            if last > 2:
                relay.forward(m, 2)
            relay.cross(m, 2)
        relay.take_wide(UP, 1)
        relay.forward_wide(UP, 1)
    for p in span:
        carried_ref[p] = jnp.zeros((PAIR, PAIR), f32)
    for s in range(last, 0, -1):

        @pl.when(z >= s)
        def _(s=s):
            onward(s).wait_recv()
            for p in span:
                carried_ref[p] = chain(
                    carried_ref[p], stack(plane_ref[s - 1, 1, p].astype(f32))
                ) + stack(plane_ref[s - 1, 0, p].astype(f32))

    for p in span:
        carried_ref[p] = chain(carried_ref[p], own_move[p]) + own_state[p]

    for i in range(1, lay.sides):
        pass_matrix(i, 0).wait_recv()
        for j in range(1, lay.cores):
            pass_matrix(i, j).start()

    def send(s):
        return pltpu.make_async_remote_copy(
            src_ref=mixed.at[s],
            dst_ref=gathered.at[s],
            send_sem=out_sem.at[s],
            recv_sem=in_sem.at[s],
            **to(tp=peers[s]),
        )

    inputs[6].wait()
    for s in range(n):
        target = peers[s] if s < n - 1 else me
        here = pl.ds(pl.multiple_of(target * rows, rows), rows)
        for p in span:
            at = slice(p * PAIR, (p + 1) * PAIR)
            outcome = local_ref[here, at] + mm(coef_ref[here, at].astype(f32), carried_ref[p], NT, 1)
            centred = outcome - head_sums(outcome) * (1.0 / PER_GROUP_DIMS)
            spread = head_sums(centred * centred) * (1.0 / PER_GROUP_DIMS)
            normed = centred * lax.rsqrt(spread + group_eps)
            reward = head_sums(
                read_ref[here, at].astype(f32) * key_ref[here, at].astype(f32) * scales_ref[:, at]
            )
            block = (
                (normed + reward * value_ref[here, at].astype(f32))
                * switch_ref[here, at].astype(f32)
            ).astype(bf16)
            if s < n - 1:
                mixed[s, :, at] = block
            else:
                gathered[s, :, at] = block
        if s < n - 1:
            send(s).start()
    if last > 2:
        relay.take_wide(UP, 2)
        relay.forward_wide(UP, 2)
        if last == 3:
            relay.take(GATE, 3)
            relay.cross(GATE, 3)
    for s in range(n - 1):
        send(s).wait_recv()
    own_matrix.wait()
    inputs[7].wait()
    for i in range(lay.sides):
        for j in range(1, lay.cores):
            pass_matrix(i, j).wait_recv()
    total = jnp.zeros((rows, width), f32)
    for i in range(lay.sides):
        for j in range(lay.cores):
            slot = lax.rem(me - place_matrix(i, j) + 2 * n - 1, n)
            total += jnp.dot(gathered[slot], matrix[i, j], preferred_element_type=f32)
    stream = skip_ref[...].astype(f32) + total.astype(bf16).astype(f32)
    stream_ref[...] = stream
    scale = lax.rsqrt(jnp.mean(stream * stream, axis=-1, keepdims=True) + norm_eps)
    mine = pl.ds(pl.multiple_of(me * rows, rows), rows)
    rows_ref[mine] = (stream * scale * gain_ref[...]).astype(bf16)
    if last:
        relay.forward(DOWN, 0)
    relay.cross(DOWN, 0)

    def pass_rows(source, target, slot):
        piece = rows_ref.at[pl.ds(pl.multiple_of(source * rows, rows), rows)]
        return pltpu.make_async_remote_copy(
            src_ref=piece,
            dst_ref=piece,
            send_sem=row_send.at[slot],
            recv_sem=row_recv.at[slot],
            **to(tp=target),
        )

    row_copies = []
    for i in range(1, lay.sides):
        copy = pass_rows(me, remote[i - 1], i * lay.cores)
        copy.start()
        row_copies.append(copy)
    for i in range(lay.sides):
        source = lax.rem(x + lay.sides - i, lay.sides) * lay.cores + c
        if i:
            row_copies[i - 1].wait_recv()
        for j in range(1, lay.cores):
            copy = pass_rows(source, partners[j - 1], i * lay.cores + j)
            copy.start()
            row_copies.append(copy)
    for r in range(3, last + 1):
        for m in (GATE, UP):
            if m == UP or last > 3:
                relay.take(m, r)
                if r < last:
                    relay.forward(m, r)
                relay.cross(m, r)
        if r < last:
            relay.take_wide(UP, r)
            relay.forward_wide(UP, r)
    for copy in row_copies[lay.sides - 1 :]:
        copy.wait_recv()

    for m in (GATE, UP):
        relay.own(m).wait()
        for lane in range(1, lay.lanes):
            for hop in range(-last, last + 1):
                if m in WIDE and hop == 0 and last:
                    continue
                taken = m in WIDE and 0 < abs(hop) < last
                relay.arrive(m, hop, lane, wide=False if taken else None)

    def down_step(r):
        if r <= last:
            relay.take(DOWN, r)
            if r < last:
                relay.forward(DOWN, r)
            relay.cross(DOWN, r)

    units = hidden_ref.shape[1]
    tile = 256 if units % 256 == 0 else 128 if units % 128 == 0 else units
    for first in range(0, units, tile):
        columns = slice(first, first + tile)
        gated = jnp.dot(rows_ref[...], whole[GATE, :, columns], preferred_element_type=f32)
        raised = jnp.dot(rows_ref[...], whole[UP, :, columns], preferred_element_type=f32)
        hidden_ref[:, columns] = (gated * jax.nn.sigmoid(gated) * raised).astype(bf16)

    relay.own(DOWN).wait()
    part = width // lay.planes
    order = list(range(1, lay.sides)) + [0]
    hops = [0] + [way * r for r in range(1, last + 1) for way in (1, -1)]

    def within(t, i, j):
        return pltpu.make_async_remote_copy(
            src_ref=inner.at[t, j - 1, i],
            dst_ref=near.at[t, j - 1, i],
            send_sem=near_send.at[t, i, j - 1],
            recv_sem=near_recv.at[t, i, j - 1],
            **to(tp=partners[j - 1]),
        )

    def between(t, i):
        return pltpu.make_async_remote_copy(
            src_ref=outer.at[t, i - 1],
            dst_ref=far.at[t, i - 1],
            send_sem=far_send.at[t, i - 1],
            recv_sem=far_recv.at[t, i - 1],
            **to(tp=remote[i - 1]),
        )

    def product(weight, i, j):
        target = lax.rem(x + i, lay.sides) * lay.cores + lax.rem(c + j, lay.cores)
        piece = hidden_ref[pl.ds(pl.multiple_of(target * rows, rows), rows)]
        return lax.dot_general(piece, weight, NT, preferred_element_type=f32)

    for t, hop in enumerate(hops):
        if hop >= 0:
            down_step(hop + 1)
        for lane in range(1, lay.lanes):
            relay.arrive(DOWN, hop, lane)

        @pl.when(relay.held(hop))
        def _(t=t, hop=hop):
            weight = whole[DOWN, pl.ds(pl.multiple_of((z - hop) * part, part), part)]
            for i in order:
                for j in range(1, lay.cores):
                    inner[t, j - 1, i] = product(weight, i, j).astype(bf16)
                    within(t, i, j).start()
            for i in order:
                own[t, i] = product(weight, i, 0)
            for i in order:
                sums = own[t, i]
                for j in range(1, lay.cores):
                    within(t, i, j).wait_recv()
                    sums += near[t, j - 1, i].astype(f32)
                if i:
                    outer[t, i - 1] = sums.astype(bf16)
                    between(t, i).start()
                else:
                    own[t, 0] = sums

    for t, hop in enumerate(hops):

        @pl.when(relay.held(hop))
        def _(t=t, hop=hop):
            columns = pl.ds(pl.multiple_of((z - hop) * part, part), part)
            sums = own[t, 0]
            for i in range(1, lay.sides):
                between(t, i).wait_recv()
                sums += far[t, i - 1].astype(f32)
            sums = sums.astype(bf16).astype(f32)
            out_ref[:, columns] = (stream_ref[:, columns] + half_step * sums).astype(bf16)

    for m in (GATE, UP, DOWN):
        relay.settle(m)
    for copy in lane_copies + row_copies:
        copy.wait_send()
    for s in range(1, lay.planes):
        pl.when(z + s < lay.planes)(onward(s).wait_send)
    for i in range(lay.sides):
        for j in range(lay.cores):
            if i or j:
                pass_matrix(i, j).wait_send()
    for s in range(n - 1):
        send(s).wait_send()
    for t, hop in enumerate(hops):

        @pl.when(relay.held(hop))
        def _(t=t):
            for i in order:
                for j in range(1, lay.cores):
                    within(t, i, j).wait_send()
                if i:
                    between(t, i).wait_send()


def per_device(
    lay,
    skip_stream,
    acceptance_signal,
    lookup_mapped,
    payload_mapped,
    result_switch,
    forget_dynamic_share,
    additive_forget_logarithm,
    forget_feature_offset,
    substitution_dynamic_share,
    substitution_feature_offset,
    diagonal_reward_scales,
    result_matrix,
    mlp_rescaler,
    switch_matrix,
    expand_matrix,
    contract_matrix,
):
    rows, width = skip_stream.shape
    length, breadth = acceptance_signal.shape
    depth, units = switch_matrix.shape
    pairs = breadth // PAIR
    n = lay.n_tp
    one = (2, pairs, PER_GROUP_DIMS, PAIR)
    lanes, planes = max(lay.lanes - 1, 1), max(lay.planes - 1, 1)
    cores, sides = max(lay.cores - 1, 1), max(lay.sides - 1, 1)
    places = (2 * lay.planes - 1) * lay.lanes
    hops = 2 * lay.planes - 1
    part = width // lay.planes
    dma = pltpu.SemaphoreType.DMA
    given = (
        acceptance_signal, lookup_mapped, payload_mapped, forget_dynamic_share,
        additive_forget_logarithm, substitution_dynamic_share, result_switch, skip_stream,
    )
    vmem, anywhere = pl.BlockSpec(memory_space=pltpu.VMEM), pl.BlockSpec(memory_space=pl.ANY)
    return pl.pallas_call(
        functools.partial(layer_kernel, lay, hops),
        in_specs=[vmem] * 4 + [anywhere] * 12,
        out_specs=vmem,
        out_shape=jax.ShapeDtypeStruct((rows, width), bf16),
        scratch_shapes=[pltpu.VMEM(array.shape, array.dtype) for array in given]
        + [
            dma((len(given),)),
            pltpu.VMEM((length, breadth), f32),
            pltpu.VMEM((length, breadth), bf16),
            pltpu.VMEM((pairs, 2 * PAIR, PAIR), f32),
            pltpu.VMEM((lay.lanes,) + one, bf16),
            pltpu.VMEM((planes,) + one, bf16),
            pltpu.VMEM(one, bf16),
            pltpu.VMEM((pairs, PAIR, PAIR), f32),
            pltpu.VMEM((n - 1, rows, breadth), bf16),
            pltpu.VMEM((n, rows, breadth), bf16),
            pltpu.VMEM((lay.sides, lay.cores, breadth, width), bf16),
            pltpu.VMEM((rows, width), f32),
            pltpu.VMEM((length, width), bf16),
            pltpu.VMEM((length, units), bf16),
            pltpu.VMEM((3, width, units), bf16),
            pltpu.VMEM((hops, lay.sides, rows, part), f32),
            pltpu.VMEM((hops, cores, lay.sides, rows, part), bf16),
            pltpu.VMEM((hops, cores, lay.sides, rows, part), bf16),
            pltpu.VMEM((hops, sides, rows, part), bf16),
            pltpu.VMEM((hops, sides, rows, part), bf16),
            dma((3, places)),
            dma((3, places)),
            dma((3,)),
            dma((lanes,)),
            dma((lanes,)),
            dma((planes,)),
            dma((planes,)),
            dma,
            dma((lay.sides, lay.cores)),
            dma((lay.sides, lay.cores)),
            dma((n,)),
            dma((n,)),
            dma((n,)),
            dma((n,)),
            dma((hops, lay.sides, cores)),
            dma((hops, lay.sides, cores)),
            dma((hops, sides)),
            dma((hops, sides)),
        ],
        compiler_params=pltpu.CompilerParams(
            collective_id=0, has_side_effects=True, vmem_limit_bytes=63 * 2**20
        ),
        cost_estimate=pl.CostEstimate(
            flops=6 * length * width * units, bytes_accessed=6 * width * units, transcendentals=0
        ),
        name="layer",
    )(
        forget_feature_offset[None, :],
        substitution_feature_offset[None, :],
        diagonal_reward_scales[None, :],
        mlp_rescaler[None, :],
        *given,
        result_matrix,
        switch_matrix,
        expand_matrix,
        contract_matrix,
    )


def solution(mesh):
    placed = (
        P(("sp", "tp"), None),
        P("sp", "tp"),
        P("sp", "tp"),
        P("sp", "tp"),
        P("sp", "tp"),
        P("sp", "tp"),
        P("sp", "tp"),
        P("tp"),
        P("sp", "tp"),
        P("tp"),
        P("tp"),
        P("tp", None),
        P(),
        P("sp", "tp"),
        P("sp", "tp"),
        P("sp", "tp"),
    )
    return jax.shard_map(
        functools.partial(per_device, Layout(mesh)),
        mesh=mesh,
        in_specs=placed,
        out_specs=P(("sp", "tp"), None),
        check_vma=False,
    )
```

```python
import functools

import jax
import jax.numpy as jnp
from jax import lax
from jax.experimental import pallas as pl
from jax.experimental.pallas import tpu as pltpu
from jax.sharding import PartitionSpec as P

PER_GROUP_DIMS = 64


norm_eps = 1e-06
group_eps = 0.00064
half_step = 0.5
exact = lax.Precision.HIGHEST

PAIR = 2 * PER_GROUP_DIMS
CHUNK = 64
ROWS_OUT = 256
NT = (((1,), (1,)), ((), ()))
NN = (((1,), (0,)), ((), ()))
TN = (((0,), (0,)), ((), ()))
bf16 = jnp.bfloat16
f32 = jnp.float32
P_SCORE, P_INV, P_SOLVE, P_OUT, P_STATE = 3, 1, 3, 3, 1


def mm(left, right, dims, passes):
    if passes == 6:
        return lax.dot_general(left, right, dims, precision=exact, preferred_element_type=f32)
    left_hi, right_hi = left.astype(bf16), right.astype(bf16)
    total = lax.dot_general(left_hi, right_hi, dims, preferred_element_type=f32)
    if passes == 3:
        left_lo = (left - left_hi.astype(f32)).astype(bf16)
        right_lo = (right - right_hi.astype(f32)).astype(bf16)
        total += lax.dot_general(left_hi, right_lo, dims, preferred_element_type=f32)
        total += lax.dot_general(left_lo, right_hi, dims, preferred_element_type=f32)
    return total


def halves(shape):
    return lax.broadcasted_iota(jnp.int32, shape, 1) < PER_GROUP_DIMS


def stack(values):
    first = halves(values.shape)
    zero = jnp.zeros_like(values)
    return jnp.concatenate([jnp.where(first, values, zero), jnp.where(first, zero, values)], 0)


def fold(values):
    size = values.shape[0] // 2
    return values[:size] + values[size:]


def head_sums(values):
    row = lax.broadcasted_iota(jnp.int32, (PAIR, PAIR), 0) // PER_GROUP_DIMS
    col = lax.broadcasted_iota(jnp.int32, (PAIR, PAIR), 1) // PER_GROUP_DIMS
    ones = jnp.where(row == col, 1.0, 0.0).astype(bf16)
    hi = values.astype(bf16)
    left = values - hi.astype(f32)
    mid = left.astype(bf16)
    low = (left - mid.astype(f32)).astype(bf16)
    return (
        jnp.dot(hi, ones, preferred_element_type=f32)
        + jnp.dot(mid, ones, preferred_element_type=f32)
        + jnp.dot(low, ones, preferred_element_type=f32)
    )


def advance_chunk(
    here, read_ref, key_ref, value_ref, forget_ref, added_ref, rate_ref, forget_off_ref,
    rate_off_ref, local_ref, coef_ref, memory,
):
    pairs = read_ref.shape[1] // PAIR
    span = range(pairs)
    row = lax.broadcasted_iota(jnp.int32, (PAIR, PAIR), 0)
    col = lax.broadcasted_iota(jnp.int32, (PAIR, PAIR), 1)
    diagonal = jnp.where(row == col, 1.0, 0.0)
    same_head = (row // CHUNK) == (col // CHUNK)
    strict = same_head & (col < row)
    inclusive = same_head & (col <= row)

    lower = (
        lax.broadcasted_iota(jnp.int32, (CHUNK, CHUNK), 1)
        <= lax.broadcasted_iota(jnp.int32, (CHUNK, CHUNK), 0)
    )
    lower = jnp.where(lower, 1.0, 0.0)
    first = halves((CHUNK, PAIR))
    at = [slice(p * PAIR, (p + 1) * PAIR) for p in span]
    decay_rate = [
        jax.nn.sigmoid(forget_off_ref[:, at[p]] + forget_ref[here, at[p]].astype(f32)) for p in span
    ]
    log_step = [
        -0.6065306597126334 * decay_rate[p]
        + jnp.where(first, added_ref[here, 2 * p : 2 * p + 1], added_ref[here, 2 * p + 1 : 2 * p + 2])
        for p in span
    ]
    cumulate = [mm(lower, log_step[p], NN, 6) for p in span]
    key = [key_ref[here, at[p]].astype(f32) for p in span]
    unit = [key[p] * lax.rsqrt(head_sums(key[p] * key[p]) + norm_eps) for p in span]
    erase = [
        unit[p] * jax.nn.sigmoid(rate_off_ref[:, at[p]] + rate_ref[here, at[p]].astype(f32))
        for p in span
    ]
    middle = [cumulate[p][CHUNK // 2 - 1 : CHUNK // 2] for p in span]
    last = [cumulate[p][CHUNK - 1 : CHUNK] for p in span]
    growth = [jnp.exp(cumulate[p] - middle[p]) for p in span]
    shrink = [jnp.exp(middle[p] - cumulate[p]) for p in span]
    to_middle = [jnp.exp(middle[p]) for p in span]
    from_middle = [jnp.exp(last[p] - middle[p]) for p in span]
    over_chunk = [jnp.exp(last[p]) for p in span]
    before = [jnp.exp(cumulate[p] - log_step[p] - middle[p]) * unit[p] for p in span]
    read = [read_ref[here, at[p]].astype(f32) * growth[p] for p in span]
    key_back = [key[p] * shrink[p] for p in span]
    erase_back = [erase[p] * shrink[p] for p in span]
    score = [
        mm(
            jnp.concatenate([stack(before[p]), stack(read[p])], 0),
            jnp.concatenate([stack(key_back[p]), stack(erase_back[p])], 0),
            NT,
            P_SCORE,
        )
        for p in span
    ]
    key_past = [jnp.where(strict, score[p][:PAIR, :PAIR], 0.0) for p in span]
    erase_past = [jnp.where(strict, score[p][:PAIR, PAIR:], 0.0) for p in span]
    key_read = [jnp.where(inclusive, score[p][PAIR:, :PAIR], 0.0) for p in span]
    erase_read = [jnp.where(inclusive, score[p][PAIR:, PAIR:], 0.0) for p in span]
    value = [stack(value_ref[here, at[p]]).astype(f32) for p in span]
    recall = [mm(key_past[p], value[p], NN, P_SOLVE) for p in span]
    inverse = [
        diagonal - jnp.where((row // 2) == (col // 2), erase_past[p], 0.0) for p in span
    ]
    size = 2
    while size < CHUNK:
        off = ((row // (2 * size)) == (col // (2 * size))) & ((row // size) != (col // size))
        part = [mm(jnp.where(off, erase_past[p], 0.0), inverse[p], NN, P_INV) for p in span]
        inverse = [inverse[p] - mm(inverse[p], part[p], NN, P_INV) for p in span]
        size *= 2
    solved = [
        mm(
            inverse[p],
            jnp.concatenate([recall[p], stack(before[p] * to_middle[p])], 1),
            NN,
            P_SOLVE,
        )
        for p in span
    ]
    inner = [
        mm(
            jnp.concatenate([key_read[p], -erase_read[p]], 1),
            jnp.concatenate(
                [jnp.concatenate([value[p], jnp.zeros_like(value[p])], 1), solved[p]], 0
            ),
            NN,
            P_OUT,
        )
        for p in span
    ]
    local = [fold(inner[p][:, :PAIR]) for p in span]
    from_start = [fold(inner[p][:, PAIR:]) + read[p] * to_middle[p] for p in span]
    both = [memory[p] for p in span]
    passed = [mm(from_start[p], both[p], NT, P_STATE) for p in span]
    for p in span:
        local_ref[here, at[p]] = local[p] + passed[p][:, :PAIR]
        coef_ref[here, at[p]] = passed[p][:, PAIR:].astype(bf16)
    key_end = [key_back[p] * from_middle[p] for p in span]
    erase_end = [erase_back[p] * from_middle[p] for p in span]
    recalled = [fold(solved[p][:, :PAIR]) for p in span]
    carried_map = [fold(solved[p][:, PAIR:]) for p in span]
    added = [
        mm(
            jnp.concatenate([value_ref[here, at[p]].astype(f32), -recalled[p]], 0),
            jnp.concatenate([key_end[p], erase_end[p]], 0),
            TN,
            P_OUT,
        )
        for p in span
    ]
    step_map = [mm(carried_map[p], erase_end[p], TN, P_OUT) for p in span]
    for p in span:
        moved = mm(both[p], jnp.where(same_head, step_map[p], 0.0), NN, P_STATE)
        kept = both[p] * over_chunk[p] - moved
        memory[p, :PAIR] = kept[:PAIR] + jnp.where(same_head, added[p], 0.0)
        memory[p, PAIR:] = kept[PAIR:]


class Layout:
    def __init__(self, mesh):
        self.n_sp, self.n_tp = mesh.shape["sp"], mesh.shape["tp"]
        devices = list(mesh.devices.flat)
        spots = [getattr(d, "coords", None) for d in devices]
        self.lanes = self.cores = 1
        if all(s is not None for s in spots):
            self.lanes = len({s[1] for s in spots})
            self.cores = len({getattr(d, "core_on_chip", 0) for d in devices})
        if self.n_sp % self.lanes:
            self.lanes = 1
        if self.n_tp % self.cores:
            self.cores = 1
        self.planes, self.sides = self.n_sp // self.lanes, self.n_tp // self.cores


def to(**where):
    return dict(device_id=where, device_id_type=pl.DeviceIdType.MESH)


def chain(total, step):
    return mm(total, step, NN, 1) + mm(total - total.astype(bf16).astype(f32), step, NN, 1)


GATE, UP, DOWN, LOW = range(4)
WIDE = (UP, LOW)
SHARE = {GATE: (0, 0, 1), UP: (1, 0, 1), DOWN: (2, 0, 2), LOW: (2, 1, 2)}


class Relay:
    def __init__(self, lay, blocks, whole, send_sem, recv_sem, own_sem):
        self.lay, self.blocks, self.whole, self.own_sem = lay, blocks, whole, own_sem
        self.send_sem, self.recv_sem = send_sem, recv_sem
        me = lax.axis_index("sp")
        self.z, self.y = me // lay.lanes, lax.rem(me, lay.lanes)
        self.depth = blocks[0].shape[0]

    def slot(self, hop, lane):
        return (hop + self.lay.planes - 1) * self.lay.lanes + lane

    def held(self, hop):
        return (self.z >= hop) & (self.z < self.lay.planes + hop)

    def wide(self, matrix, hop):
        if matrix not in WIDE:
            return False
        first, last = self.z == hop, self.z == self.lay.planes - 1 + hop
        return first | last if hop == 0 else first if hop > 0 else last

    def part(self, matrix, hop, lane):
        source = (self.z - hop) * self.lay.lanes + lax.rem(
            self.y + self.lay.lanes - lane, self.lay.lanes
        )
        array, share, shares = SHARE[matrix]
        size = self.depth // shares
        first = pl.multiple_of(source * self.depth + share * size, size)
        return self.whole.at[array, pl.ds(first, size)]

    def block(self, matrix):
        array, share, shares = SHARE[matrix]
        size = self.depth // shares
        return self.blocks[array].at[pl.ds(share * size, size)]

    def copy(self, matrix, source, place, plane, lane):
        return pltpu.make_async_remote_copy(
            src_ref=self.block(matrix) if source == (0, 0) else self.part(matrix, *source),
            dst_ref=self.part(matrix, *source),
            send_sem=self.send_sem.at[matrix, self.slot(*place)],
            recv_sem=self.recv_sem.at[matrix, self.slot(*place)],
            **to(sp=plane * self.lay.lanes + lane),
        )

    def ahead(self, matrix, hop, way, lane=0):
        there = self.z + way
        wanted = self.held(hop) & (there >= 0) & (there < self.lay.planes)
        if lane:
            wanted = wanted & self.wide(matrix, hop)
        return self.copy(matrix, (hop, lane), (hop + way, lane), there, self.y), wanted

    def aside(self, matrix, hop, lane):
        beside = lax.rem(self.y + lane, self.lay.lanes)
        wanted = self.held(hop)
        if hop and matrix in WIDE:
            wanted = wanted & ~self.wide(matrix, hop)
        return self.copy(matrix, (hop, 0), (hop, lane), self.z, beside), wanted

    def start(self, pair):
        pl.when(pair[1])(pair[0].start)

    def own(self, matrix):
        return pltpu.make_async_copy(
            self.block(matrix), self.part(matrix, 0, 0), self.own_sem.at[matrix]
        )

    def arrive(self, matrix, hop, lane, wide=None):
        piece = self.part(matrix, hop, lane)
        slot = self.slot(hop, lane)
        wait = pltpu.make_async_remote_copy(
            src_ref=piece,
            dst_ref=piece,
            send_sem=self.send_sem.at[matrix, slot],
            recv_sem=self.recv_sem.at[matrix, slot],
            **to(sp=lax.axis_index("sp")),
        ).wait_recv
        wanted = self.held(hop)
        if wide is not None and matrix in WIDE:
            wanted = wanted & (self.wide(matrix, hop) if wide else ~self.wide(matrix, hop))
        pl.when(wanted)(wait)

    def take(self, matrix, reach):
        for hop in (reach, -reach):
            self.arrive(matrix, hop, 0)

    def forward(self, matrix, reach):
        for way in (1, -1):
            self.start(self.ahead(matrix, way * reach, way))

    def take_wide(self, matrix, reach):
        for hop in (reach, -reach):
            for lane in range(1, self.lay.lanes):
                self.arrive(matrix, hop, lane, wide=True)

    def forward_wide(self, matrix, reach):
        for way in (1, -1):
            for lane in range(1, self.lay.lanes):
                self.start(self.ahead(matrix, way * reach, way, lane))

    def cross(self, matrix, reach):
        for hop in (reach, -reach) if reach else (0,):
            for lane in range(1, self.lay.lanes):
                self.start(self.aside(matrix, hop, lane))

    def settle(self, matrix):
        last = self.lay.planes - 1
        for reach in range(last + 1):
            for way in (1, -1):
                if reach < last:
                    for lane in range(self.lay.lanes if matrix in WIDE else 1):
                        copy, wanted = self.ahead(matrix, way * reach, way, lane)
                        pl.when(wanted)(copy.wait_send)
            for hop in (reach, -reach) if reach else (0,):
                for lane in range(1, self.lay.lanes):
                    copy, wanted = self.aside(matrix, hop, lane)
                    pl.when(wanted)(copy.wait_send)


def layer_kernel(lay, steps, *refs):
    forget_off_ref, rate_off_ref, scales_ref, gain_ref, *given = refs[:16]
    given, (matrix_ref, gate_ref, up_ref, down_ref) = given[:8], given[8:12]
    out_ref = refs[16]
    loaded = refs[17:25]
    read_ref, key_ref, value_ref, forget_ref, heads_ref, rate_ref, switch_ref, skip_ref = loaded
    (
        input_sem, added_ref,
        local_ref, coef_ref, memory, lane_ref, plane_ref, mine_ref, carried_ref, mixed, gathered,
        matrix, stream_ref, rows_ref, hidden_ref, whole, own, inner, near, outer, far,
        relay_send, relay_recv, own_sem, lane_send, lane_recv, plane_send, plane_recv,
        load_sem, matrix_send, matrix_recv, out_sem, in_sem, row_send, row_recv,
        near_send, near_recv, far_send, far_recv,
    ) = refs[25:]
    n = lay.n_tp
    rows, width = skip_ref.shape
    length, breadth = read_ref.shape
    pairs = breadth // PAIR
    span = range(pairs)
    last = lay.planes - 1
    spot, me = lax.axis_index("sp"), lax.axis_index("tp")
    z, y = spot // lay.lanes, lax.rem(spot, lay.lanes)
    x, c = me // lay.cores, lax.rem(me, lay.cores)
    beside = [z * lay.lanes + lax.rem(y + s, lay.lanes) for s in range(1, lay.lanes)]
    line = [lax.rem(spot + s * lay.lanes, lay.n_sp) for s in range(1, lay.planes)]
    peers = [lax.rem(me + s, n) for s in range(1, n)]
    partners = [x * lay.cores + lax.rem(c + j, lay.cores) for j in range(1, lay.cores)]
    remote = [lax.rem(x + i, lay.sides) * lay.cores + c for i in range(1, lay.sides)]

    barrier = pltpu.get_barrier_semaphore()
    for axis, others in (("sp", beside + line), ("tp", peers)):
        for other in others:
            pl.semaphore_signal(barrier, inc=1, **to(**{axis: other}))
    pl.semaphore_wait(barrier, len(beside) + len(line) + len(peers))

    relay = Relay(lay, (gate_ref, up_ref, down_ref), whole, relay_send, relay_recv, own_sem)
    for m in (GATE, UP):
        relay.forward(m, 0) if last else None
        relay.cross(m, 0)

    def place_matrix(i, j):
        side, core = lax.rem(x + lay.sides - i, lay.sides), lax.rem(c + lay.cores - j, lay.cores)
        return side * lay.cores + core

    def pass_matrix(i, j):
        source = matrix_ref if i == 0 or j == 0 else matrix.at[i, 0]
        target = partners[j - 1] if j else remote[i - 1]
        return pltpu.make_async_remote_copy(
            src_ref=source,
            dst_ref=matrix.at[i, j],
            send_sem=matrix_send.at[i, j],
            recv_sem=matrix_recv.at[i, j],
            **to(tp=target),
        )

    inputs = [
        pltpu.make_async_copy(given[k], loaded[k], input_sem.at[k]) for k in range(len(given))
    ]
    for copy in inputs:
        copy.start()
    own_matrix = pltpu.make_async_copy(matrix_ref, matrix.at[0, 0], load_sem)
    own_matrix.start()
    for i in range(1, lay.sides):
        pass_matrix(i, 0).start()
    for j in range(1, lay.cores):
        pass_matrix(0, j).start()

    for m in SHARE:
        relay.own(m).start()
    diagonal = jnp.where(
        lax.broadcasted_iota(jnp.int32, (PAIR, PAIR), 0)
        == lax.broadcasted_iota(jnp.int32, (PAIR, PAIR), 1),
        1.0,
        0.0,
    )
    for p in span:
        memory[p, :PAIR] = jnp.zeros((PAIR, PAIR), f32)
        memory[p, PAIR:] = diagonal

    chunks = length // CHUNK
    for copy in inputs[:6]:
        copy.wait()
    added_ref[...] = heads_ref[...].T

    def gate_aside(first):
        for lane in range(1, lay.lanes):
            for hop, wanted in ((1, z > 0), (-1, z == 0)) if first else ((-1, z > 0),):
                copy, held = relay.aside(GATE, hop, lane)
                relay.start((copy, held & wanted))

    def one(turn, _):
        if last:

            @pl.when(turn == 5 * chunks // 12)
            def _():
                relay.take(GATE, 1)
                if last > 1:
                    relay.forward(GATE, 1)
                gate_aside(True)

            @pl.when(turn == 10 * chunks // 12)
            def _():
                relay.take(UP, 1)
                if last > 1:
                    relay.forward(UP, 1)
                for lane in range(1, lay.lanes):
                    relay.arrive(UP, 0, lane)
                relay.forward_wide(UP, 0)
                relay.cross(LOW, 0)

        here = pl.ds(pl.multiple_of(turn * CHUNK, CHUNK), CHUNK)
        advance_chunk(
            here, read_ref, key_ref, value_ref, forget_ref, added_ref, rate_ref, forget_off_ref,
            rate_off_ref, local_ref, coef_ref, memory,
        )
        return 0

    lax.fori_loop(0, chunks, one, 0)

    for p in span:
        lane_ref[y, 0, p] = fold(memory[p, :PAIR]).astype(bf16)
        lane_ref[y, 1, p] = fold(memory[p, PAIR:]).astype(bf16)
    lane_copies = [
        pltpu.make_async_remote_copy(
            src_ref=lane_ref.at[y],
            dst_ref=lane_ref.at[y],
            send_sem=lane_send.at[s],
            recv_sem=lane_recv.at[s],
            **to(sp=other),
        )
        for s, other in enumerate(beside)
    ]
    for copy in lane_copies:
        copy.start()
    if last:
        gate_aside(False)
        relay.cross(UP, 1)
    for copy in lane_copies:
        copy.wait_recv()
    state = [stack(lane_ref[0, 0, p].astype(f32)) for p in span]
    move = [stack(lane_ref[0, 1, p].astype(f32)) for p in span]
    own_state = [jnp.where(y > 0, state[p], 0.0) for p in span]
    own_move = [jnp.where(y > 0, move[p], diagonal) for p in span]
    for t in range(1, lay.lanes):
        for p in span:
            step = stack(lane_ref[t, 1, p].astype(f32))
            state[p] = chain(state[p], step) + stack(lane_ref[t, 0, p].astype(f32))
            move[p] = chain(move[p], step)
            if t < lay.lanes - 1:
                own_state[p] = jnp.where(y > t, state[p], own_state[p])
                own_move[p] = jnp.where(y > t, move[p], own_move[p])
    onward = pltpu.make_async_remote_copy(
        src_ref=mine_ref,
        dst_ref=plane_ref,
        send_sem=plane_send,
        recv_sem=plane_recv,
        **to(sp=lax.rem(spot + lay.lanes, lay.n_sp)),
    )

    def pass_on(carried):
        for p in span:
            total = state[p] if carried is None else chain(carried[p], move[p]) + state[p]
            mine_ref[p] = fold(total).astype(bf16)
        onward.start()

    if last:
        pl.when(z == 0)(functools.partial(pass_on, None))
    if last > 1:
        for m in (GATE, UP):
            relay.take(m, 2)
            if last > 2:
                relay.forward(m, 2)
            relay.cross(m, 2)
        relay.take_wide(UP, 1)
        relay.forward_wide(UP, 1)
    for p in span:
        carried_ref[p] = own_state[p]
    if last:

        @pl.when(z > 0)
        def _():
            onward.wait_recv()
            carried = [stack(plane_ref[p].astype(f32)) for p in span]

            @pl.when(z < last)
            def _():
                pass_on(carried)

            for p in span:
                carried_ref[p] = chain(carried[p], own_move[p]) + own_state[p]

    for i in range(1, lay.sides):
        pass_matrix(i, 0).wait_recv()
        for j in range(1, lay.cores):
            pass_matrix(i, j).start()

    def send(s):
        return pltpu.make_async_remote_copy(
            src_ref=mixed.at[s],
            dst_ref=gathered.at[s],
            send_sem=out_sem.at[s],
            recv_sem=in_sem.at[s],
            **to(tp=peers[s]),
        )

    inputs[6].wait()
    for s in range(n):
        target = peers[s] if s < n - 1 else me
        here = pl.ds(pl.multiple_of(target * rows, rows), rows)
        for p in span:
            at = slice(p * PAIR, (p + 1) * PAIR)
            outcome = local_ref[here, at] + mm(coef_ref[here, at].astype(f32), carried_ref[p], NT, 1)
            centred = outcome - head_sums(outcome) * (1.0 / PER_GROUP_DIMS)
            spread = head_sums(centred * centred) * (1.0 / PER_GROUP_DIMS)
            normed = centred * lax.rsqrt(spread + group_eps)
            reward = head_sums(
                read_ref[here, at].astype(f32) * key_ref[here, at].astype(f32) * scales_ref[:, at]
            )
            block = (
                (normed + reward * value_ref[here, at].astype(f32))
                * switch_ref[here, at].astype(f32)
            ).astype(bf16)
            if s < n - 1:
                mixed[s, :, at] = block
            else:
                gathered[s, :, at] = block
        if s < n - 1:
            send(s).start()
    if last > 2:
        relay.take_wide(UP, 2)
        relay.forward_wide(UP, 2)
        if last == 3:
            relay.take(GATE, 3)
            relay.cross(GATE, 3)
    for s in range(n - 1):
        send(s).wait_recv()
    own_matrix.wait()
    inputs[7].wait()
    for i in range(lay.sides):
        for j in range(1, lay.cores):
            pass_matrix(i, j).wait_recv()
    total = jnp.zeros((rows, width), f32)
    for i in range(lay.sides):
        for j in range(lay.cores):
            slot = lax.rem(me - place_matrix(i, j) + 2 * n - 1, n)
            total += jnp.dot(gathered[slot], matrix[i, j], preferred_element_type=f32)
    stream = skip_ref[...].astype(f32) + total.astype(bf16).astype(f32)
    stream_ref[...] = stream
    scale = lax.rsqrt(jnp.mean(stream * stream, axis=-1, keepdims=True) + norm_eps)
    mine = pl.ds(pl.multiple_of(me * rows, rows), rows)
    rows_ref[mine] = (stream * scale * gain_ref[...]).astype(bf16)
    if last:
        relay.forward(DOWN, 0)
        relay.forward(LOW, 0)
    relay.cross(DOWN, 0)
    if last:
        for lane in range(1, lay.lanes):
            relay.arrive(LOW, 0, lane)
        relay.forward_wide(LOW, 0)
    else:
        relay.cross(LOW, 0)

    def pass_rows(source, target, slot):
        piece = rows_ref.at[pl.ds(pl.multiple_of(source * rows, rows), rows)]
        return pltpu.make_async_remote_copy(
            src_ref=piece,
            dst_ref=piece,
            send_sem=row_send.at[slot],
            recv_sem=row_recv.at[slot],
            **to(tp=target),
        )

    row_copies = []
    for i in range(1, lay.sides):
        copy = pass_rows(me, remote[i - 1], i * lay.cores)
        copy.start()
        row_copies.append(copy)
    for i in range(lay.sides):
        source = lax.rem(x + lay.sides - i, lay.sides) * lay.cores + c
        if i:
            row_copies[i - 1].wait_recv()
        for j in range(1, lay.cores):
            copy = pass_rows(source, partners[j - 1], i * lay.cores + j)
            copy.start()
            row_copies.append(copy)
    for r in range(3, last + 1):
        for m in (GATE, UP):
            if m == UP or last > 3:
                relay.take(m, r)
                if r < last:
                    relay.forward(m, r)
                relay.cross(m, r)
        if r < last:
            relay.take_wide(UP, r)
            relay.forward_wide(UP, r)
    for copy in row_copies[lay.sides - 1 :]:
        copy.wait_recv()

    for m in (GATE, UP):
        relay.own(m).wait()
        for lane in range(1, lay.lanes):
            for hop in range(-last, last + 1):
                if m in WIDE and hop == 0 and last:
                    continue
                taken = m in WIDE and 0 < abs(hop) < last
                relay.arrive(m, hop, lane, wide=False if taken else None)

    def down_step(r):
        if r > last:
            return
        if r > 1:
            relay.take_wide(LOW, r - 1)
            relay.forward_wide(LOW, r - 1)
        for m in (DOWN, LOW):
            relay.take(m, r)
            if r < last:
                relay.forward(m, r)
            relay.cross(m, r)

    units = hidden_ref.shape[1]
    tile = 256 if units % 256 == 0 else 128 if units % 128 == 0 else units
    for first in range(0, units, tile):
        columns = slice(first, first + tile)
        gated = jnp.dot(rows_ref[...], whole[GATE, :, columns], preferred_element_type=f32)
        raised = jnp.dot(rows_ref[...], whole[UP, :, columns], preferred_element_type=f32)
        hidden_ref[:, columns] = (gated * jax.nn.sigmoid(gated) * raised).astype(bf16)

    relay.own(DOWN).wait()
    relay.own(LOW).wait()
    part = width // lay.planes
    order = list(range(1, lay.sides)) + [0]
    hops = [0] + [way * r for r in range(1, last + 1) for way in (1, -1)]

    def within(t, i, j):
        return pltpu.make_async_remote_copy(
            src_ref=inner.at[t, j - 1, i],
            dst_ref=near.at[t, j - 1, i],
            send_sem=near_send.at[t, i, j - 1],
            recv_sem=near_recv.at[t, i, j - 1],
            **to(tp=partners[j - 1]),
        )

    def between(t, i):
        return pltpu.make_async_remote_copy(
            src_ref=outer.at[t, i - 1],
            dst_ref=far.at[t, i - 1],
            send_sem=far_send.at[t, i - 1],
            recv_sem=far_recv.at[t, i - 1],
            **to(tp=remote[i - 1]),
        )

    def product(weight, i, j):
        target = lax.rem(x + i, lay.sides) * lay.cores + lax.rem(c + j, lay.cores)
        piece = hidden_ref[pl.ds(pl.multiple_of(target * rows, rows), rows)]
        return lax.dot_general(piece, weight, NT, preferred_element_type=f32)

    for t, hop in enumerate(hops):
        if hop >= 0:
            down_step(hop + 1)
        for lane in range(1, lay.lanes):
            relay.arrive(DOWN, hop, lane)
            if hop or not last:
                taken = 0 < abs(hop) < last
                relay.arrive(LOW, hop, lane, wide=False if taken else None)

        @pl.when(relay.held(hop))
        def _(t=t, hop=hop):
            weight = whole[DOWN, pl.ds(pl.multiple_of((z - hop) * part, part), part)]
            for i in order:
                for j in range(1, lay.cores):
                    inner[t, j - 1, i] = product(weight, i, j).astype(bf16)
                    within(t, i, j).start()
            for i in order:
                own[t, i] = product(weight, i, 0)
            for i in order:
                sums = own[t, i]
                for j in range(1, lay.cores):
                    within(t, i, j).wait_recv()
                    sums += near[t, j - 1, i].astype(f32)
                if i:
                    outer[t, i - 1] = sums.astype(bf16)
                    between(t, i).start()
                else:
                    own[t, 0] = sums

    for t, hop in enumerate(hops):

        @pl.when(relay.held(hop))
        def _(t=t, hop=hop):
            columns = pl.ds(pl.multiple_of((z - hop) * part, part), part)
            sums = own[t, 0]
            for i in range(1, lay.sides):
                between(t, i).wait_recv()
                sums += far[t, i - 1].astype(f32)
            sums = sums.astype(bf16).astype(f32)
            out_ref[:, columns] = (stream_ref[:, columns] + half_step * sums).astype(bf16)

    for m in SHARE:
        relay.settle(m)
    for copy in lane_copies + row_copies:
        copy.wait_send()
    if last:
        pl.when(z < last)(onward.wait_send)
    for i in range(lay.sides):
        for j in range(lay.cores):
            if i or j:
                pass_matrix(i, j).wait_send()
    for s in range(n - 1):
        send(s).wait_send()
    for t, hop in enumerate(hops):

        @pl.when(relay.held(hop))
        def _(t=t):
            for i in order:
                for j in range(1, lay.cores):
                    within(t, i, j).wait_send()
                if i:
                    between(t, i).wait_send()


def per_device(
    lay,
    skip_stream,
    acceptance_signal,
    lookup_mapped,
    payload_mapped,
    result_switch,
    forget_dynamic_share,
    additive_forget_logarithm,
    forget_feature_offset,
    substitution_dynamic_share,
    substitution_feature_offset,
    diagonal_reward_scales,
    result_matrix,
    mlp_rescaler,
    switch_matrix,
    expand_matrix,
    contract_matrix,
):
    rows, width = skip_stream.shape
    length, breadth = acceptance_signal.shape
    depth, units = switch_matrix.shape
    pairs = breadth // PAIR
    n = lay.n_tp
    one = (2, pairs, PER_GROUP_DIMS, PAIR)
    lanes = max(lay.lanes - 1, 1)
    cores, sides = max(lay.cores - 1, 1), max(lay.sides - 1, 1)
    places = (2 * lay.planes - 1) * lay.lanes
    hops = 2 * lay.planes - 1
    part = width // lay.planes
    dma = pltpu.SemaphoreType.DMA
    given = (
        acceptance_signal, lookup_mapped, payload_mapped, forget_dynamic_share,
        additive_forget_logarithm.T, substitution_dynamic_share, result_switch, skip_stream,
    )
    vmem, anywhere = pl.BlockSpec(memory_space=pltpu.VMEM), pl.BlockSpec(memory_space=pl.ANY)
    return pl.pallas_call(
        functools.partial(layer_kernel, lay, hops),
        in_specs=[vmem] * 4 + [anywhere] * 12,
        out_specs=vmem,
        out_shape=jax.ShapeDtypeStruct((rows, width), bf16),
        scratch_shapes=[pltpu.VMEM(array.shape, array.dtype) for array in given]
        + [
            dma((len(given),)),
            pltpu.VMEM(additive_forget_logarithm.shape, f32),
            pltpu.VMEM((length, breadth), f32),
            pltpu.VMEM((length, breadth), bf16),
            pltpu.VMEM((pairs, 2 * PAIR, PAIR), f32),
            pltpu.VMEM((lay.lanes,) + one, bf16),
            pltpu.VMEM(one[1:], bf16),
            pltpu.VMEM(one[1:], bf16),
            pltpu.VMEM((pairs, PAIR, PAIR), f32),
            pltpu.VMEM((n - 1, rows, breadth), bf16),
            pltpu.VMEM((n, rows, breadth), bf16),
            pltpu.VMEM((lay.sides, lay.cores, breadth, width), bf16),
            pltpu.VMEM((rows, width), f32),
            pltpu.VMEM((length, width), bf16),
            pltpu.VMEM((length, units), bf16),
            pltpu.VMEM((3, width, units), bf16),
            pltpu.VMEM((hops, lay.sides, rows, part), f32),
            pltpu.VMEM((hops, cores, lay.sides, rows, part), bf16),
            pltpu.VMEM((hops, cores, lay.sides, rows, part), bf16),
            pltpu.VMEM((hops, sides, rows, part), bf16),
            pltpu.VMEM((hops, sides, rows, part), bf16),
            dma((len(SHARE), places)),
            dma((len(SHARE), places)),
            dma((len(SHARE),)),
            dma((lanes,)),
            dma((lanes,)),
            dma,
            dma,
            dma,
            dma((lay.sides, lay.cores)),
            dma((lay.sides, lay.cores)),
            dma((n,)),
            dma((n,)),
            dma((n,)),
            dma((n,)),
            dma((hops, lay.sides, cores)),
            dma((hops, lay.sides, cores)),
            dma((hops, sides)),
            dma((hops, sides)),
        ],
        compiler_params=pltpu.CompilerParams(
            collective_id=0, has_side_effects=True, vmem_limit_bytes=63 * 2**20
        ),
        cost_estimate=pl.CostEstimate(
            flops=6 * length * width * units, bytes_accessed=6 * width * units, transcendentals=0
        ),
        name="layer",
    )(
        forget_feature_offset[None, :],
        substitution_feature_offset[None, :],
        diagonal_reward_scales[None, :],
        mlp_rescaler[None, :],
        *given,
        result_matrix,
        switch_matrix,
        expand_matrix,
        contract_matrix,
    )


def solution(mesh):
    placed = (
        P(("sp", "tp"), None),
        P("sp", "tp"),
        P("sp", "tp"),
        P("sp", "tp"),
        P("sp", "tp"),
        P("sp", "tp"),
        P("sp", "tp"),
        P("tp"),
        P("sp", "tp"),
        P("tp"),
        P("tp"),
        P("tp", None),
        P(),
        P("sp", "tp"),
        P("sp", "tp"),
        P("sp", "tp"),
    )
    return jax.shard_map(
        functools.partial(per_device, Layout(mesh)),
        mesh=mesh,
        in_specs=placed,
        out_specs=P(("sp", "tp"), None),
        check_vma=False,
    )
```
